32 devices in a mesh: dp: 4 (over y, x), kv: 4 (over z), tp: 2 (over core).
Axes of the slice: x: 2, y: 2, z: 4, core: 2. Of those that a mesh axis runs over, the one named last changes fastest.
Arguments:
- tokens: bfloat16 [16, 4096], P('dp', 'kv'), may hold values from -24 to 24
- positions: int32 [16], P(('dp', 'kv')), may hold values from 0 to 4095
- state: float32 [16, 16, 128, 128], P(('dp', 'kv'), 'tp'), may hold values from -0.6 to 0.6
- w_query: bfloat16 [4096, 2048], P('kv', 'tp'), may hold values from -0.09375 to 0.09375
- w_key: bfloat16 [4096, 2048], P('kv', 'tp'), may hold values from -0.09375 to 0.09375
- w_value: bfloat16 [4096, 2048], P('kv', 'tp'), may hold values from -0.09375 to 0.09375
- w_gate: bfloat16 [4096, 2048], P('kv', 'tp'), may hold values from -0.09375 to 0.09375
- w_out: bfloat16 [2048, 4096], P(None, ('kv', 'tp')), may hold values from -0.25 to 0.25
- gain_mix: float32 [4096], replicated, may hold values from 0.1 to 1.9
- w_ffn_gate: bfloat16 [4096, 11008], P(None, ('kv', 'tp')), may hold values from -0.09375 to 0.09375
- w_ffn_up: bfloat16 [4096, 11008], P(None, ('kv', 'tp')), may hold values from -0.09375 to 0.09375
- w_ffn_down: bfloat16 [11008, 4096], P(('kv', 'tp')), may hold values from -0.109375 to 0.109375
- gain_out: float32 [4096], replicated, may hold values from 0.1 to 1.9
Outputs:
- layer_out: bfloat16 [16, 4096], P('dp', ('kv', 'tp'))
- new_state: float32 [16, 16, 128, 128], P(('dp', 'kv'), 'tp')
The draws below stay inside these ranges and needn't reach their ends.
All inputs are finite; a program needn't handle non-finite values.
Results may differ from the reference program's by a relative error of at most 0.018.
Values may be sent and summed in bfloat16 or wider, within the bound.
A program may use at most 128 MiB of HBM per device.

```python
import jax
import jax.numpy as jnp
from jax import lax

D = 4096
HEADS = 16
HEAD_DIM = 128
FF = 11008
BATCH = 16


def draw_tokens(key, part):
    normal_key = jax.random.fold_in(jax.random.fold_in(key, 11), 0)
    columns = jnp.arange(D, dtype=jnp.float32) / D
    column_scale = 0.5 * 4.0 ** columns
    base = jnp.clip(jax.random.normal(normal_key, (BATCH, D), jnp.float32), -6.0, 6.0)
    values = base * column_scale[None, :]
    return jnp.clip(values, -24.0, 24.0).astype(jnp.bfloat16)


def with_ends(entries, rng, least, top_value):
    shape = entries.shape
    place = [jax.random.randint(jax.random.fold_in(rng, axis), (), 0, shape[axis]) for axis in range(len(shape))]
    entries = entries.at[tuple(place)].set(least)
    longest = shape.index(max(shape))
    place[longest] = (place[longest] + 1) % shape[longest]
    return entries.at[tuple(place)].set(top_value)


def block_levels(own_key, dims, cuts, low, largest):
    def one(position, shards_of):
        steps = jax.random.uniform(jax.random.fold_in(jax.random.fold_in(own_key, 6), position), (shards_of,), jnp.float32, low / len(cuts), largest / len(cuts))
        return jnp.repeat(jnp.exp(steps), dims[position] // shards_of).reshape((-1,) + (1,) * (len(dims) - position - 1))

    level = one(*cuts[0])
    for cut in cuts[1:]:
        level = level * one(*cut)
    return level


def normal_values(rng, shape, scale, bound, cuts=(), held_as=jnp.bfloat16):
    values = jax.random.normal(rng, shape, jnp.float32) * scale
    if len(cuts) > 0:
        values = block_levels(rng, shape, cuts, -0.22, 0.18) * values
    return jnp.clip(values, min=-bound, max=bound).astype(held_as)


def setup_inputs(seed: int = 0) -> dict:
    seeds = jax.random.split(jax.random.key(seed), 14)
    return {
        "tokens": draw_tokens(jax.random.fold_in(seeds[13], 71), 0),
        "positions": with_ends(jax.random.randint(seeds[1], (BATCH,), 0, 4096), jax.random.fold_in(seeds[1], 1), 0, 4095).astype(jnp.int32),
        "state": normal_values(seeds[2], (BATCH, HEADS, HEAD_DIM, HEAD_DIM), 0.1, 0.6, ((0, 16), (1, 2)), jnp.float32),
        "w_query": normal_values(seeds[3], (D, HEADS * HEAD_DIM), D ** -0.5, 0.09375, ((0, 4), (1, 2))),
        "w_key": normal_values(seeds[4], (D, HEADS * HEAD_DIM), D ** -0.5, 0.09375, ((0, 4), (1, 2))),
        "w_value": normal_values(seeds[5], (D, HEADS * HEAD_DIM), D ** -0.5, 0.09375, ((0, 4), (1, 2))),
        "w_gate": normal_values(seeds[6], (D, HEADS * HEAD_DIM), D ** -0.5, 0.09375, ((0, 4), (1, 2))),
        "w_out": normal_values(seeds[7], (HEADS * HEAD_DIM, D), (HEADS * HEAD_DIM // 4) ** -0.5, 0.25, ((1, 8),)),
        "gain_mix": jnp.clip(1.0 + 0.18 * jax.random.normal(seeds[8], (D,), jnp.float32), 0.1, 1.9),
        "w_ffn_gate": normal_values(seeds[9], (D, FF), D ** -0.5, 0.09375, ((1, 8),)),
        "w_ffn_up": normal_values(seeds[10], (D, FF), D ** -0.5, 0.09375, ((1, 8),)),
        "w_ffn_down": normal_values(seeds[11], (FF, D), (FF // 4) ** -0.5, 0.109375, ((0, 8),)),
        "gain_out": jnp.clip(1.0 + 0.18 * jax.random.normal(seeds[12], (D,), jnp.float32), 0.1, 1.9),
    }


def rotate(vectors, positions):
    half = vectors.shape[-1] // 2
    inverse = 10000.0 ** (-jnp.arange(half, dtype=jnp.float32) / half)
    angle = positions.astype(jnp.float32)[:, None, None] * inverse[None, None, :]
    cosine = jnp.cos(angle)
    sine = jnp.sin(angle)
    first = vectors[..., :half]
    second = vectors[..., half:]
    return jnp.concatenate([first * cosine - second * sine, first * sine + second * cosine], -1)

def layer_norm(values, gain):
    count = values.shape[-1]
    mean = lax.optimization_barrier(jnp.sum(values, -1, keepdims=True)) / count
    var = lax.optimization_barrier(jnp.sum(values * values, -1, keepdims=True)) / count - mean * mean
    return (values - mean) * lax.rsqrt(var + 1e-05) * gain

def reference(tokens, positions, state, w_query, w_key, w_value, w_gate, w_out, gain_mix, w_ffn_gate, w_ffn_up, w_ffn_down, gain_out):
    rows = tokens.shape[0]
    heads = state.shape[1]
    width_head = state.shape[2]
    query = jnp.dot(tokens, w_query, preferred_element_type=jnp.float32).reshape(rows, heads, width_head)
    key = jnp.dot(tokens, w_key, preferred_element_type=jnp.float32).reshape(rows, heads, width_head)
    value = jnp.dot(tokens, w_value, preferred_element_type=jnp.float32).reshape(rows, heads, width_head)
    gate_pre = jnp.dot(tokens, w_gate, preferred_element_type=jnp.float32)
    query = rotate(query, positions)
    key = rotate(key, positions) * width_head ** (-0.5)
    head_ids = jnp.arange(heads, dtype=jnp.float32)
    decay = 1.0 - 2.0 ** (-5.0 - 6.0 * head_ids / (heads - 1))
    new_state = decay[None, :, None, None] * state + key[:, :, :, None] * value[:, :, None, :]
    retained = jnp.einsum('bhd,bhdv->bhv', query, new_state, precision=lax.Precision.HIGHEST)
    mean = lax.optimization_barrier(jnp.mean(retained, -1, keepdims=True))
    var = lax.optimization_barrier(jnp.mean(jnp.square(retained - mean), -1, keepdims=True))
    normed = (retained - mean) * lax.rsqrt(var + 1e-05)
    attended = (normed.reshape(rows, heads * width_head) * jax.nn.silu(gate_pre)).astype(jnp.bfloat16)
    mixed = jnp.dot(attended, w_out, preferred_element_type=jnp.float32)
    mixed_pre = (tokens.astype(jnp.float32) + mixed).astype(jnp.bfloat16)
    hidden = layer_norm(mixed_pre.astype(jnp.float32), gain_mix).astype(jnp.bfloat16)
    gate = jnp.dot(hidden, w_ffn_gate, preferred_element_type=jnp.float32)
    upward = jnp.dot(hidden, w_ffn_up, preferred_element_type=jnp.float32)
    inner = (jax.nn.silu(gate) * upward).astype(jnp.bfloat16)
    ffn = jnp.dot(inner, w_ffn_down, preferred_element_type=jnp.float32)
    layer_out = layer_norm(hidden.astype(jnp.float32) + ffn, gain_out).astype(jnp.bfloat16)
    return (layer_out, new_state)
```

```python
import functools

import jax
import jax.numpy as jnp
import numpy as np
from jax import lax
from jax.experimental import pallas as pl
from jax.experimental.pallas import tpu as pltpu
from jax.sharding import PartitionSpec as P

MESH = pl.DeviceIdType.MESH
F32 = jnp.float32
BF16 = jnp.bfloat16


def dot_rows(values, weight):
    return lax.dot_general(values, weight, (((1,), (1,)), ((), ())), preferred_element_type=F32)


def near_first(kv, count):
    low = jnp.minimum(kv, count - 1 - kv)
    step = jnp.where(2 * kv < count, 1, -1)
    order = []
    for k in range(1, count):
        offset = jnp.where(
            k <= 2 * low, (k + 1) // 2 * (1 if k % 2 == 0 else -1), (k - low) * step
        )
        order.append(kv + offset)
    return order


def step_kernel(kv_count, tp_count, *refs):
    operands = 14

    def body(local_sem, q_send_sem, q_recv_sem, send_sem, recv_sem):
        step_body(
            kv_count, tp_count, *refs, local_sem, q_send_sem, q_recv_sem, send_sem, recv_sem
        )

    group = kv_count * tp_count
    pl.run_scoped(
        body,
        pltpu.SemaphoreType.DMA((operands,)),
        pltpu.SemaphoreType.DMA((4, kv_count)),
        pltpu.SemaphoreType.DMA((4, kv_count)),
        pltpu.SemaphoreType.DMA((4, group)),
        pltpu.SemaphoreType.DMA((4, group)),
    )


def step_body(
    kv_count,
    tp_count,
    tok_h,
    pos_h,
    state_h,
    wq_h,
    wk_h,
    wv_h,
    wg_h,
    wout_h,
    gmix_h,
    wfg_h,
    wfu_h,
    wfd_h,
    gout_h,
    inv_h,
    out_v,
    nst,
    tok,
    pos,
    state,
    wq,
    wk,
    wv,
    wg,
    wout,
    gmix,
    wfg,
    wfu,
    wfd,
    gout,
    inv,
    qsend,
    qrecv,
    att,
    att_rows,
    mix,
    gain_rows,
    acc_gate,
    acc_up,
    inner,
    fsend,
    frecv,
    sums,
    local_sem,
    q_send_sem,
    q_recv_sem,
    send_sem,
    recv_sem,
):
    group = kv_count * tp_count
    dp = lax.axis_index("dp")
    kv = lax.axis_index("kv")
    tp = lax.axis_index("tp")
    me = kv * tp_count + tp
    rows = tok.shape[0]
    heads = state.shape[0]
    width_head = state.shape[1]
    width = wfg.shape[1]
    cols = mix.shape[2]
    ff = wfg.shape[0]

    near = near_first(kv, kv_count)
    beside = [lax.rem(tp + e, tp_count) for e in range(1, tp_count)]
    far_peers = [(chip, core) for chip in reversed(near) for core in range(tp_count)]
    near_peers = [(kv, core) for core in beside]
    near_peers += [(chip, core) for chip in near for core in range(tp_count)]

    barrier = pltpu.get_barrier_semaphore()
    for chip, core in far_peers + [(kv, core) for core in beside]:
        pl.semaphore_signal(barrier, inc=1, device_id=(dp, chip, core), device_id_type=MESH)

    loads = []

    def load(src, dst):
        copy = pltpu.make_async_copy(src, dst, local_sem.at[len(loads)])
        copy.start()
        loads.append(copy)
        return copy

    tok_load = load(tok_h, tok)
    pos_load = load(pos_h, pos)
    inv_load = load(inv_h, inv)
    proj_loads = [
        load(src, dst) for src, dst in ((wq_h, wq), (wk_h, wk), (wv_h, wv), (wg_h, wg))
    ]
    state_load = load(state_h, state)
    gmix_load = load(gmix_h, gmix)
    gout_load = load(gout_h, gout)

    pos_load.wait()
    inv_load.wait()
    lane = lax.broadcasted_iota(jnp.int32, (1, width_head), 1)
    angle = pos[...].astype(F32) * inv[...]
    cosine = jnp.cos(angle)
    sine = jnp.sin(angle)
    sine = jnp.where(lane < width_head // 2, -sine, sine)

    tok_load.wait()
    later = []
    q_copies = []

    def send_part(p):
        for d in range(kv_count - 1, 0, -1):
            chip = near[d - 1]
            copy = pltpu.make_async_remote_copy(
                src_ref=qsend.at[chip, p],
                dst_ref=qrecv.at[kv, p],
                send_sem=q_send_sem.at[p, d],
                recv_sem=q_recv_sem.at[p, kv],
                device_id=(dp, chip, tp),
                device_id_type=MESH,
            )
            copy.start()
            q_copies.append(copy)

    following = ((wout_h, wout), (wfg_h, wfg), (wfu_h, wfu), (wfd_h, wfd))
    for p, weight in enumerate((wq, wk, wv, wg)):
        proj_loads[p].wait()
        later.append(load(*following[p]))
        part = jnp.dot(tok[...], weight[...], preferred_element_type=F32)
        for i in range(kv_count):
            for h in range(heads):
                qsend[i, p, h : h + 1, :] = part[
                    i : i + 1, h * width_head : (h + 1) * width_head
                ]
        if p == 2:
            pl.semaphore_wait(barrier, group - 1)
            for done in range(3):
                send_part(done)
        elif p == 3:
            send_part(p)
    wout_load, wfg_load, wfu_load, wfd_load = later

    head_id = (tp * heads + lax.broadcasted_iota(jnp.int32, (heads, width_head), 0)).astype(F32)
    total_heads = heads * tp_count
    decay = 1.0 - jnp.exp2(-5.0 - 6.0 * head_id / (total_heads - 1))

    gmix_load.wait()
    gain = gmix[...]
    gain_high = gain.astype(BF16).astype(F32)
    row_id = lax.broadcasted_iota(jnp.int32, (8, width), 0)
    gain_rows[...] = jnp.where(
        row_id == rows, gain_high, jnp.where(row_id == rows + 1, gain - gain_high, 0.0)
    )

    def rotate_row(x):
        return x * cosine + pltpu.roll(x, width_head // 2, 1) * sine

    def collect(p):
        total = qsend[kv, p]
        for chip in near:
            pltpu.make_async_remote_copy(
                src_ref=qsend.at[chip, p],
                dst_ref=qrecv.at[chip, p],
                send_sem=q_send_sem.at[p, 0],
                recv_sem=q_recv_sem.at[p, chip],
                device_id=(dp, chip, tp),
                device_id_type=MESH,
            ).wait_recv()
            total = total + qrecv[chip, p]
        return total

    state_load.wait()
    query = rotate_row(collect(0))
    query_t = jnp.transpose(query)
    held = jnp.concatenate(
        [
            jnp.sum(query_t[:, h : h + 1] * state[h], axis=0, keepdims=True)
            for h in range(heads)
        ],
        axis=0,
    )
    key = rotate_row(collect(1)) * width_head ** (-0.5)
    match = jnp.sum(query * key, axis=1, keepdims=True)
    value = collect(2)
    retained = decay * held + match * value
    mean = jnp.mean(retained, -1, keepdims=True)
    var = jnp.mean(jnp.square(retained - mean), -1, keepdims=True)
    normed = (retained - mean) * lax.rsqrt(var + 1e-05)
    gate_pre = collect(3)
    silu_gate = gate_pre / (1.0 + jnp.exp(-gate_pre))
    att[me] = (normed * silu_gate).astype(BF16)

    def remote(phase, src, dst, slot, chip, core):
        return pltpu.make_async_remote_copy(
            src_ref=src,
            dst_ref=dst,
            send_sem=send_sem.at[phase, slot],
            recv_sem=recv_sem.at[phase, me],
            device_id=(dp, chip, core),
            device_id_type=MESH,
        )

    def send_all(phase, ref):
        copies = []
        for chip, core in far_peers + [(kv, core) for core in beside]:
            copy = remote(phase, ref.at[me], ref.at[me], len(copies), chip, core)
            copy.start()
            copies.append(copy)
        return copies

    def wait_from(phase, ref, chip, core):
        source = chip * tp_count + core
        pltpu.make_async_remote_copy(
            src_ref=ref.at[me],
            dst_ref=ref.at[source],
            send_sem=send_sem.at[phase, 0],
            recv_sem=recv_sem.at[phase, source],
            device_id=(dp, chip, core),
            device_id_type=MESH,
        ).wait_recv()

    att_copies = send_all(0, att)

    key_t = jnp.transpose(key)
    for h in range(heads):
        nst[h] = decay[h : h + 1, :] * state[h] + key_t[:, h : h + 1] * value[h : h + 1, :]

    wout_load.wait()
    for chip, core in near_peers:
        wait_from(0, att, chip, core)
    for p in range(group):
        att_rows[p * heads : (p + 1) * heads, :] = att[p].astype(F32)
    lhs = jnp.concatenate(
        [
            att_rows[pl.ds(t * heads + h, rows, stride=tp_count * heads), :]
            for t in range(tp_count)
            for h in range(heads)
        ],
        axis=1,
    ).astype(BF16)
    mixed = jnp.dot(lhs, wout[...], preferred_element_type=F32)
    tok_own = tok[:, pl.ds(pl.multiple_of(tp * cols, cols), cols)]
    own = (tok_own.astype(F32) + mixed).astype(BF16)
    mix[me] = own
    mix_copies = send_all(1, mix)

    own = own.astype(F32)
    shift = jnp.mean(own, 1, keepdims=True)
    gout_load.wait()
    wfg_load.wait()
    wfu_load.wait()
    tile = 256
    starts = list(range(0, ff, tile))
    own_lanes = pl.ds(pl.multiple_of(me * cols, cols), cols)

    def centred(x, lanes):
        z = jnp.concatenate([x * gmix[:, lanes], jnp.zeros((8 - rows, x.shape[1]), F32)], 0)
        return (z + gain_rows[:, lanes]).astype(BF16)

    def up_part(lhs, lanes, first):
        for start in starts:
            at = pl.ds(start, min(tile, ff - start))
            for weight, acc in ((wfg, acc_gate), (wfu, acc_up)):
                part = dot_rows(lhs, weight[at, lanes])
                acc[:, at] = part if first else acc[:, at] + part

    own = own - shift
    up_part(centred(own, own_lanes), own_lanes, True)
    total = own
    squares = own * own
    for core in beside:
        wait_from(1, mix, kv, core)
        lanes = pl.ds(pl.multiple_of((kv * tp_count + core) * cols, cols), cols)
        x = mix[kv * tp_count + core].astype(F32) - shift
        total = total + x
        squares = squares + x * x
        up_part(centred(x, lanes), lanes, False)
    for chip in near:
        for core in range(tp_count):
            wait_from(1, mix, chip, core)
        pieces = []
        for core in range(tp_count):
            lanes = pl.ds(pl.multiple_of((chip * tp_count + core) * cols, cols), cols)
            x = mix[chip * tp_count + core].astype(F32) - shift
            total = total + x
            squares = squares + x * x
            pieces.append(centred(x, lanes))
        lanes = pl.ds(pl.multiple_of(chip * (tp_count * cols), tp_count * cols), tp_count * cols)
        up_part(jnp.concatenate(pieces, 1), lanes, False)

    mean = jnp.sum(total, 1, keepdims=True) / width
    var = jnp.sum(squares, 1, keepdims=True) / width - mean * mean
    scale = lax.rsqrt(var + 1e-05)
    hid_own = ((own - mean) * scale * gmix[:, own_lanes]).astype(BF16).astype(F32)

    def finish(acc, at):
        bias = acc[rows : rows + 1, at] + acc[rows + 1 : rows + 2, at]
        return scale * (acc[:rows, at] - mean * bias)

    for start in starts:
        at = pl.ds(start, min(tile, ff - start))
        gate = finish(acc_gate, at)
        inner[:, at] = (gate / (1.0 + jnp.exp(-gate)) * finish(acc_up, at)).astype(BF16)

    wfd_load.wait()
    main = ff // 128 * 128

    def down_part(at):
        result = jnp.dot(inner[:, :main], wfd[:main, at], preferred_element_type=F32)
        if main < ff:
            result += jnp.dot(inner[:, main:], wfd[main:, at], preferred_element_type=F32)
        return result

    f_copies = []

    def send_down(chip, core, result):
        owner = chip * tp_count + core
        fsend[owner] = result.astype(BF16)
        copy = remote(2, fsend.at[owner], frecv.at[me], len(f_copies), chip, core)
        copy.start()
        f_copies.append(copy)

    for chip in reversed(near):
        span = tp_count * cols
        both = down_part(pl.ds(pl.multiple_of(chip * span, span), span))
        for core in range(tp_count):
            send_down(chip, core, both[:, core * cols : (core + 1) * cols])
    for core in beside:
        lanes = pl.ds(pl.multiple_of((kv * tp_count + core) * cols, cols), cols)
        send_down(kv, core, down_part(lanes))
    summed = hid_own + down_part(own_lanes)
    for chip, core in near_peers:
        wait_from(2, frecv, chip, core)
        summed = summed + frecv[chip * tp_count + core].astype(F32)
    own_sum = jnp.sum(summed, 1, keepdims=True)
    own_square = jnp.sum(summed * summed, 1, keepdims=True)
    low_half = lax.broadcasted_iota(jnp.int32, (rows, 128), 1) < 64
    sums[me] = jnp.where(low_half, own_sum, own_square)
    sum_copies = send_all(3, sums)
    for chip, core in near_peers:
        wait_from(3, sums, chip, core)
    all_sums = functools.reduce(lambda a, b: a + b, [sums[p] for p in range(group)])
    mean = all_sums[:, :1] / width
    var = all_sums[:, 64:65] / width - mean * mean
    gain = gout[:, own_lanes]
    out_v[...] = ((summed - mean) * lax.rsqrt(var + 1e-05) * gain).astype(BF16)

    for copies in (q_copies, att_copies, mix_copies, f_copies, sum_copies):
        for copy in copies:
            copy.wait_send()


def store_kernel(out_v, nst_v, out_h, nst_h, sem):
    copies = [
        pltpu.make_async_copy(nst_v, nst_h, sem.at[0]),
        pltpu.make_async_copy(out_v, out_h, sem.at[1]),
    ]
    for copy in copies:
        copy.start()
    for copy in copies:
        copy.wait()


def fused_step(
    tokens,
    positions,
    state,
    w_query,
    w_key,
    w_value,
    w_gate,
    w_out,
    gain_mix,
    w_ffn_gate,
    w_ffn_up,
    w_ffn_down,
    gain_out,
):
    kv_count = lax.axis_size("kv")
    tp_count = lax.axis_size("tp")
    group = kv_count * tp_count
    rows = tokens.shape[0]
    _, heads, width_head, _ = state.shape
    width = w_ffn_gate.shape[0]
    cols = w_out.shape[1]
    half = width_head // 2
    inverse = 10000.0 ** (-np.arange(half, dtype=np.float32) / half)
    inverse = np.tile(inverse.astype(np.float32), 2)[None, :]
    arrays = (
        tokens,
        positions[None, :],
        state[0],
        w_query,
        w_key,
        w_value,
        w_gate,
        w_out,
        gain_mix[None, :],
        w_ffn_gate.T,
        w_ffn_up.T,
        w_ffn_down,
        gain_out[None, :],
        jnp.asarray(inverse),
    )
    held = [pltpu.VMEM(a.shape, a.dtype) for a in arrays]
    vmem_spec = pl.BlockSpec(memory_space=pltpu.VMEM)
    any_spec = pl.BlockSpec(memory_space=pl.ANY)
    out, new_state = pl.pallas_call(
        functools.partial(step_kernel, kv_count, tp_count),
        out_shape=(
            pltpu.VMEM((rows, cols), BF16),
            pltpu.VMEM(state.shape[1:], F32),
        ),
        in_specs=[any_spec] * len(arrays),
        out_specs=(vmem_spec, vmem_spec),
        scratch_shapes=held
        + [
            pltpu.VMEM((kv_count, 4, heads, width_head), F32),
            pltpu.VMEM((kv_count, 4, heads, width_head), F32),
            pltpu.VMEM((group, heads, width_head), BF16),
            pltpu.VMEM((group * heads, width_head), F32),
            pltpu.VMEM((group, rows, cols), BF16),
            pltpu.VMEM((8, width), F32),
            pltpu.VMEM((8, w_ffn_gate.shape[1]), F32),
            pltpu.VMEM((8, w_ffn_gate.shape[1]), F32),
            pltpu.VMEM((rows, w_ffn_gate.shape[1]), BF16),
            pltpu.VMEM((group, rows, cols), BF16),
            pltpu.VMEM((group, rows, cols), BF16),
            pltpu.VMEM((group, rows, 128), F32),
        ],
        compiler_params=pltpu.CompilerParams(
            collective_id=0, has_side_effects=True, vmem_limit_bytes=56 * 2**20
        ),
    )(*arrays)
    out, new_state = pl.pallas_call(
        store_kernel,
        out_shape=(
            jax.ShapeDtypeStruct(out.shape, out.dtype),
            jax.ShapeDtypeStruct(new_state.shape, new_state.dtype),
        ),
        in_specs=[vmem_spec, vmem_spec],
        out_specs=(any_spec, any_spec),
        scratch_shapes=[pltpu.SemaphoreType.DMA((2,))],
        compiler_params=pltpu.CompilerParams(vmem_limit_bytes=2**20),
    )(out, new_state)
    return out, new_state[None]


def fits_kernel(tokens, state, w_out, kv_count, tp_count):
    seqs, _, width_head, _ = state.shape
    return (
        seqs == 1
        and width_head == 128
        and w_out.shape[1] % 128 == 0
        and tokens.shape[0] == kv_count
        and kv_count <= 6
        and kv_count * tp_count <= 16
    )


def rotate(vectors, positions):
    half = vectors.shape[-1] // 2
    inverse = 10000.0 ** (-jnp.arange(half, dtype=jnp.float32) / half)
    angle = positions.astype(jnp.float32)[:, None, None] * inverse[None, None, :]
    cosine = jnp.cos(angle)
    sine = jnp.sin(angle)
    first = vectors[..., :half]
    second = vectors[..., half:]
    return jnp.concatenate([first * cosine - second * sine, first * sine + second * cosine], -1)


def finish_norm(values, sums, squares, count, gain):
    mean = sums / count
    var = squares / count - mean * mean
    return (values - mean[:, None]) * lax.rsqrt(var + 1e-05)[:, None] * gain[None, :]


def on_device(
    tokens,
    positions,
    state,
    w_query,
    w_key,
    w_value,
    w_gate,
    w_out,
    gain_mix,
    w_ffn_gate,
    w_ffn_up,
    w_ffn_down,
    gain_out,
):
    if fits_kernel(tokens, state, w_out, lax.axis_size("kv"), lax.axis_size("tp")):
        return fused_step(
            tokens,
            positions,
            state,
            w_query,
            w_key,
            w_value,
            w_gate,
            w_out,
            gain_mix,
            w_ffn_gate,
            w_ffn_up,
            w_ffn_down,
            gain_out,
        )
    seqs = state.shape[0]
    heads = state.shape[1]
    width_head = state.shape[2]
    proj_cols = w_query.shape[1]
    width = w_ffn_gate.shape[0]
    cols = w_out.shape[1]
    group_rows = tokens.shape[0]
    kv_count = lax.axis_size("kv")
    tp_count = lax.axis_size("tp")
    tp_index = lax.axis_index("tp")
    col_start = (lax.axis_index("kv") * tp_count + tp_index) * cols
    projected = lax.psum_scatter(
        jnp.concatenate(
            [
                jnp.dot(tokens, w_query, preferred_element_type=jnp.float32),
                jnp.dot(tokens, w_key, preferred_element_type=jnp.float32),
                jnp.dot(tokens, w_value, preferred_element_type=jnp.float32),
                jnp.dot(tokens, w_gate, preferred_element_type=jnp.float32),
            ],
            axis=1,
        ),
        "kv",
        scatter_dimension=0,
        tiled=True,
    )
    query = projected[:, :proj_cols].reshape(seqs, heads, width_head)
    key = projected[:, proj_cols : 2 * proj_cols].reshape(seqs, heads, width_head)
    value = projected[:, 2 * proj_cols : 3 * proj_cols].reshape(seqs, heads, width_head)
    gate_pre = projected[:, 3 * proj_cols :]
    query = rotate(query, positions)
    key = rotate(key, positions) * width_head ** (-0.5)
    total_heads = heads * tp_count
    head_ids = (tp_index * heads + jnp.arange(heads, dtype=jnp.int32)).astype(jnp.float32)
    decay = 1.0 - 2.0 ** (-5.0 - 6.0 * head_ids / (total_heads - 1))
    new_state = decay[None, :, None, None] * state + key[:, :, :, None] * value[:, :, None, :]
    retained = jnp.einsum("bhd,bhdv->bhv", query, new_state, precision=lax.Precision.HIGHEST)
    mean = jnp.mean(retained, -1, keepdims=True)
    var = jnp.mean(jnp.square(retained - mean), -1, keepdims=True)
    normed = (retained - mean) * lax.rsqrt(var + 1e-05)
    attended = (normed.reshape(seqs, proj_cols) * jax.nn.silu(gate_pre)).astype(jnp.bfloat16)
    gathered = lax.all_gather(attended[None], ("kv", "tp"), axis=0, tiled=True)
    gathered = gathered.reshape(kv_count, tp_count, seqs, proj_cols)
    out_blocks = w_out.reshape(tp_count, proj_cols, cols)
    mixed = jnp.einsum(
        "itsc,tcd->isd", gathered, out_blocks, preferred_element_type=jnp.float32
    ).reshape(group_rows, cols)
    tokens_own = lax.dynamic_slice_in_dim(tokens, tp_index * cols, cols, 1)
    mixed_pre = (tokens_own.astype(jnp.float32) + mixed).astype(jnp.bfloat16)
    gain_out_own = lax.dynamic_slice_in_dim(gain_out, col_start, cols, 0)
    whole_rows = lax.all_gather(mixed_pre, ("kv", "tp"), axis=1, tiled=True).astype(jnp.float32)
    hidden = finish_norm(
        whole_rows, jnp.sum(whole_rows, 1), jnp.sum(whole_rows * whole_rows, 1), width, gain_mix
    ).astype(jnp.bfloat16)
    hidden_own = lax.dynamic_slice_in_dim(hidden, col_start, cols, 1)
    gate = jnp.dot(hidden, w_ffn_gate, preferred_element_type=jnp.float32)
    upward = jnp.dot(hidden, w_ffn_up, preferred_element_type=jnp.float32)
    inner = (jax.nn.silu(gate) * upward).astype(jnp.bfloat16)
    ffn_cols = lax.psum_scatter(
        lax.dot_general(
            w_ffn_down, inner, (((0,), (1,)), ((), ())), preferred_element_type=jnp.float32
        ),
        ("kv", "tp"),
        scatter_dimension=0,
        tiled=True,
    )
    summed = hidden_own.astype(jnp.float32) + ffn_cols.T
    out_sums, out_squares = lax.psum(
        (jnp.sum(summed, 1), jnp.sum(summed * summed, 1)), ("kv", "tp")
    )
    layer_out = finish_norm(summed, out_sums, out_squares, width, gain_out_own).astype(jnp.bfloat16)
    return (layer_out, new_state)


def solution(mesh):
    return jax.shard_map(
        on_device,
        mesh=mesh,
        in_specs=(
            P("dp", "kv"),
            P(("dp", "kv")),
            P(("dp", "kv"), "tp", None, None),
            P("kv", "tp"),
            P("kv", "tp"),
            P("kv", "tp"),
            P("kv", "tp"),
            P(None, ("kv", "tp")),
            P(),
            P(None, ("kv", "tp")),
            P(None, ("kv", "tp")),
            P(("kv", "tp"), None),
            P(),
        ),
        out_specs=(P("dp", ("kv", "tp")), P(("dp", "kv"), "tp", None, None)),
        check_vma=False,
    )
```

```python
import functools

import jax
import jax.numpy as jnp
import numpy as np
from jax import lax
from jax.experimental import pallas as pl
from jax.experimental.pallas import tpu as pltpu
from jax.sharding import PartitionSpec as P

MESH = pl.DeviceIdType.MESH
F32 = jnp.float32
BF16 = jnp.bfloat16


def dot_rows(values, weight):
    return lax.dot_general(values, weight, (((1,), (1,)), ((), ())), preferred_element_type=F32)


def nearest(kv, count, k):
    low = jnp.minimum(kv, count - 1 - kv)
    step = jnp.where(2 * kv < count, 1, -1)
    side = 1 - 2 * (k % 2)
    return kv + jnp.where(k <= 2 * low, (k + 1) // 2 * side, (k - low) * step)


def step_kernel(kv_count, tp_count, *refs):
    def body(*sems):
        step_body(kv_count, tp_count, *refs, *sems)

    group = kv_count * tp_count
    pl.run_scoped(
        body,
        pltpu.SemaphoreType.DMA((13,)),
        pltpu.SemaphoreType.DMA((kv_count, 2)),
        pltpu.SemaphoreType.DMA((4, kv_count)),
        pltpu.SemaphoreType.DMA((4, kv_count)),
        pltpu.SemaphoreType.DMA((4, group)),
        pltpu.SemaphoreType.DMA((4, group)),
    )


def step_body(
    kv_count,
    tp_count,
    tok_h,
    pos_h,
    state_h,
    wq_h,
    wk_h,
    wv_h,
    wg_h,
    wout_h,
    gmix_h,
    wfg_h,
    wfu_h,
    wfd_h,
    gout_h,
    inv_h,
    out_v,
    nst,
    tok,
    pos,
    state,
    wq,
    wk,
    wv,
    wg,
    wout,
    gmix,
    w_up,
    wfd,
    gout,
    inv,
    qsend,
    qrecv,
    half_part,
    mixed_part,
    att,
    att_rows,
    mix,
    gain_rows,
    acc_gate,
    acc_up,
    turned,
    eye,
    inner,
    fsend,
    frecv,
    sums,
    local_sem,
    up_sem,
    q_send_sem,
    q_recv_sem,
    send_sem,
    recv_sem,
):
    group = kv_count * tp_count
    dp = lax.axis_index("dp")
    kv = lax.axis_index("kv")
    tp = lax.axis_index("tp")
    me = kv * tp_count + tp
    rows = tok.shape[0]
    heads = state.shape[0]
    width_head = state.shape[1]
    width = w_up.shape[2]
    cols = mix.shape[2]
    ff = w_up.shape[1]

    near = [nearest(kv, kv_count, k) for k in range(1, kv_count)]
    beside = [lax.rem(tp + e, tp_count) for e in range(1, tp_count)]
    far_peers = [(chip, core) for chip in reversed(near) for core in range(tp_count)]
    near_peers = [(kv, core) for core in beside]
    near_peers += [(chip, core) for chip in near for core in range(tp_count)]

    loads = []

    def load(src, dst):
        copy = pltpu.make_async_copy(src, dst, local_sem.at[len(loads)])
        copy.start()
        loads.append(copy)
        return copy

    tok_load = load(tok_h, tok)
    pos_load = load(pos_h, pos)
    inv_load = load(inv_h, inv)
    deep = wg.shape[0] // 2
    halves = [pl.ds(0, deep), pl.ds(deep, deep)]
    proj_loads = [[load(src, dst)] for src, dst in ((wq_h, wq), (wk_h, wk), (wv_h, wv))]
    proj_loads.append([load(wg_h.at[half], wg.at[half]) for half in halves])
    state_load = load(state_h, state)
    gmix_load = load(gmix_h, gmix)
    gout_load = load(gout_h, gout)

    barrier = pltpu.get_barrier_semaphore()
    for chip, core in far_peers + [(kv, core) for core in beside]:
        pl.semaphore_signal(barrier, inc=1, device_id=(dp, chip, core), device_id_type=MESH)

    pos_load.wait()
    inv_load.wait()
    lane = lax.broadcasted_iota(jnp.int32, (1, width_head), 1)
    eye[...] = jnp.where(
        lax.broadcasted_iota(jnp.int32, eye.shape, 0)
        == lax.broadcasted_iota(jnp.int32, eye.shape, 1),
        1.0,
        0.0,
    ).astype(BF16)
    angle = pos[...].astype(F32) * inv[...]
    cosine = jnp.cos(angle)
    sine = jnp.sin(angle)
    sine = jnp.where(lane < width_head // 2, -sine, sine)

    tok_load.wait()
    later = []

    def part_copies(p):
        return [
            pltpu.make_async_remote_copy(
                src_ref=qsend.at[chip, p],
                dst_ref=qrecv.at[kv, p],
                send_sem=q_send_sem.at[p, d],
                recv_sem=q_recv_sem.at[p, kv],
                device_id=(dp, chip, tp),
                device_id_type=MESH,
            )
            for d, chip in reversed(list(enumerate(near)))
        ]

    span = tp_count * cols

    def chip_lanes(chip):
        return pl.ds(pl.multiple_of(chip * span, span), span)

    def up_copy(rank, m):
        chip = nearest(kv, kv_count, kv_count - 1 - rank)
        at = chip_lanes(chip)
        source = (wfg_h, wfu_h)[m] if isinstance(m, int) else wfg_h
        return pltpu.make_async_copy(source.at[:, at], w_up.at[m, :, at], up_sem.at[rank, m])

    stage = jnp.minimum(kv_count - 1 - kv, 3)
    for p, weight in enumerate((wq, wk, wv, wg)):
        proj_loads[p][0].wait()
        if p == 0:
            later.append(load(wout_h, wout))
        ranks = [p] if p < 3 else list(range(3, kv_count))
        for rank in ranks:
            for m in range(2):
                up_copy(rank, m).start()
        if p < 3:
            part = jnp.dot(tok[...], weight[...], preferred_element_type=F32)
        else:
            later.append(load(wfd_h, wfd))
            half_part[...] = jnp.dot(
                tok[:, :deep], weight[:deep], preferred_element_type=F32
            )
            proj_loads[p][1].wait()
            part = half_part[...] + jnp.dot(
                tok[:, deep:], weight[deep:], preferred_element_type=F32
            )
        for i in range(kv_count):
            for h in range(heads):
                qsend[i, p, h : h + 1, :] = part[
                    i : i + 1, h * width_head : (h + 1) * width_head
                ]

        @pl.when(stage == p)
        def first_sends():
            pl.semaphore_wait(barrier, group - 1)
            for done in range(p + 1):
                for copy in part_copies(done):
                    copy.start()

        if p > 0:

            @pl.when(stage < p)
            def next_send():
                for copy in part_copies(p):
                    copy.start()

    wout_load, wfd_load = later

    head_id = (tp * heads + lax.broadcasted_iota(jnp.int32, (heads, width_head), 0)).astype(F32)
    total_heads = heads * tp_count
    decay = 1.0 - jnp.exp2(-5.0 - 6.0 * head_id / (total_heads - 1))

    gmix_load.wait()
    gain = gmix[...]
    gain_high = gain.astype(BF16).astype(F32)
    row_id = lax.broadcasted_iota(jnp.int32, (8, width), 0)
    gain_rows[...] = jnp.where(
        row_id == rows, gain_high, jnp.where(row_id == rows + 1, gain - gain_high, 0.0)
    )

    def rotate_row(x):
        return x * cosine + pltpu.roll(x, width_head // 2, 1) * sine

    def collect(p):
        total = qsend[kv, p]
        for chip in near:
            pltpu.make_async_remote_copy(
                src_ref=qsend.at[chip, p],
                dst_ref=qrecv.at[chip, p],
                send_sem=q_send_sem.at[p, 0],
                recv_sem=q_recv_sem.at[p, chip],
                device_id=(dp, chip, tp),
                device_id_type=MESH,
            ).wait_recv()
            total = total + qrecv[chip, p]
        return total

    pieces = 2 * (kv_count - 1)
    turned_early = functools.reduce(
        lambda a, b: a + b,
        [jnp.where(kv == c, max(pieces // (c + 1) - 1 + min(c, 1), 0), 0) for c in range(kv_count - 1)],
    )

    def turn(piece, carry):
        rank = piece // 2
        m = piece % 2
        up_copy(rank, m).wait()
        start = nearest(kv, kv_count, kv_count - 1 - rank) * span
        for k in range(0, span, 512):
            for f in range(0, ff, 256):
                n = min(256, ff - f)
                at = pl.ds(pl.multiple_of(start + k, 256), 256)
                turned[piece, k : k + 256, f : f + n] = dot_rows(
                    eye[...], w_up[m, f : f + n, at]
                ).astype(BF16)
                if k + 256 < span:
                    at = pl.ds(pl.multiple_of(start + k + 256, 256), 256)
                    turned[piece, k + 256 : k + 512, f : f + n] = w_up[m, f : f + n, at].T
        return carry

    lax.fori_loop(0, turned_early, turn, 0)

    state_load.wait()
    query = rotate_row(collect(0))
    query_t = jnp.transpose(query)
    held = jnp.concatenate(
        [
            jnp.sum(query_t[:, h : h + 1] * state[h], axis=0, keepdims=True)
            for h in range(heads)
        ],
        axis=0,
    )
    key = rotate_row(collect(1)) * width_head ** (-0.5)
    match = jnp.sum(query * key, axis=1, keepdims=True)
    value = collect(2)
    retained = decay * held + match * value
    mean = jnp.mean(retained, -1, keepdims=True)
    var = jnp.mean(jnp.square(retained - mean), -1, keepdims=True)
    normed = (retained - mean) * lax.rsqrt(var + 1e-05)
    gate_pre = collect(3)
    silu_gate = gate_pre / (1.0 + jnp.exp(-gate_pre))
    att[me] = (normed * silu_gate).astype(BF16)

    def remote(phase, src, dst, slot, chip, core):
        return pltpu.make_async_remote_copy(
            src_ref=src,
            dst_ref=dst,
            send_sem=send_sem.at[phase, slot],
            recv_sem=recv_sem.at[phase, me],
            device_id=(dp, chip, core),
            device_id_type=MESH,
        )

    def send_all(phase, ref):
        copies = []
        for chip, core in far_peers + [(kv, core) for core in beside]:
            copy = remote(phase, ref.at[me], ref.at[me], len(copies), chip, core)
            copy.start()
            copies.append(copy)
        return copies

    def wait_from(phase, ref, chip, core):
        source = chip * tp_count + core
        pltpu.make_async_remote_copy(
            src_ref=ref.at[me],
            dst_ref=ref.at[source],
            send_sem=send_sem.at[phase, 0],
            recv_sem=recv_sem.at[phase, source],
            device_id=(dp, chip, core),
            device_id_type=MESH,
        ).wait_recv()

    att_copies = send_all(0, att)

    key_t = jnp.transpose(key)
    for h in range(heads):
        nst[h] = decay[h : h + 1, :] * state[h] + key_t[:, h : h + 1] * value[h : h + 1, :]

    lax.fori_loop(turned_early, pieces, turn, 0)

    wout_load.wait()
    mixed = None
    for t in reversed(range(tp_count)):
        for chip in near:
            wait_from(0, att, chip, t)

        @pl.when(tp != t)
        def wait_beside():
            wait_from(0, att, kv, t)

        for i in range(kv_count):
            start = (i * tp_count + t) * heads
            att_rows[start : start + heads, :] = att[i * tp_count + t].astype(F32)
        lhs = jnp.concatenate(
            [
                att_rows[pl.ds(t * heads + h, rows, stride=tp_count * heads), :]
                for h in range(heads)
            ],
            axis=1,
        ).astype(BF16)
        depth = heads * width_head
        part = jnp.dot(lhs, wout[t * depth : (t + 1) * depth], preferred_element_type=F32)
        if t > 0:
            if t < tp_count - 1:
                part = part + mixed_part[...]
            mixed_part[...] = part
        else:
            mixed = part + mixed_part[...]
    tok_own = tok[:, pl.ds(pl.multiple_of(tp * cols, cols), cols)]
    own = (tok_own.astype(F32) + mixed).astype(BF16)
    mix[me] = own
    mix_copies = send_all(1, mix)

    own = own.astype(F32)
    shift = jnp.mean(own, 1, keepdims=True)
    gout_load.wait()
    for m in range(2):
        up_copy(kv_count - 1, m).wait()
    tile = 256
    starts = list(range(0, ff, tile))
    own_lanes = pl.ds(pl.multiple_of(me * cols, cols), cols)

    def centred(x, lanes):
        z = jnp.concatenate([x * gmix[:, lanes], jnp.zeros((8 - rows, x.shape[1]), F32)], 0)
        return (z + gain_rows[:, lanes]).astype(BF16)

    def up_turned(lhs, rank):
        for start in starts:
            at = pl.ds(start, min(tile, ff - start))
            for m, acc in enumerate((acc_gate, acc_up)):
                acc[:, at] += jnp.dot(
                    lhs, turned[2 * rank + m, :, at], preferred_element_type=F32
                )

    def up_part(lhs, lanes, first):
        for start in starts:
            at = pl.ds(start, min(tile, ff - start))
            for m, acc in enumerate((acc_gate, acc_up)):
                part = dot_rows(lhs, w_up[m, at, lanes])
                acc[:, at] = part if first else acc[:, at] + part

    own = own - shift
    up_part(centred(own, own_lanes), own_lanes, True)
    total = own
    squares = own * own
    for core in beside:
        wait_from(1, mix, kv, core)
        lanes = pl.ds(pl.multiple_of((kv * tp_count + core) * cols, cols), cols)
        x = mix[kv * tp_count + core].astype(F32) - shift
        total = total + x
        squares = squares + x * x
        up_part(centred(x, lanes), lanes, False)
    for k, chip in enumerate(near):
        for core in range(tp_count):
            wait_from(1, mix, chip, core)
        if k == kv_count - 2:
            wfd_load.wait()
        blocks = []
        for core in range(tp_count):
            lanes = pl.ds(pl.multiple_of((chip * tp_count + core) * cols, cols), cols)
            x = mix[chip * tp_count + core].astype(F32) - shift
            total = total + x
            squares = squares + x * x
            blocks.append(centred(x, lanes))
        up_turned(jnp.concatenate(blocks, 1), kv_count - 2 - k)

    mean = jnp.sum(total, 1, keepdims=True) / width
    var = jnp.sum(squares, 1, keepdims=True) / width - mean * mean
    scale = lax.rsqrt(var + 1e-05)
    hid_own = ((own - mean) * scale * gmix[:, own_lanes]).astype(BF16).astype(F32)

    def finish(acc, at):
        bias = acc[rows : rows + 1, at] + acc[rows + 1 : rows + 2, at]
        return scale * (acc[:rows, at] - mean * bias)

    for start in starts:
        at = pl.ds(start, min(tile, ff - start))
        gate = finish(acc_gate, at)
        inner[:, at] = (gate / (1.0 + jnp.exp(-gate)) * finish(acc_up, at)).astype(BF16)

    main = ff // 128 * 128

    def down_part(at):
        result = jnp.dot(inner[:, :main], wfd[:main, at], preferred_element_type=F32)
        if main < ff:
            result += jnp.dot(inner[:, main:], wfd[main:, at], preferred_element_type=F32)
        return result

    f_copies = []

    def send_down(chip, core, result):
        owner = chip * tp_count + core
        fsend[owner] = result.astype(BF16)
        copy = remote(2, fsend.at[owner], frecv.at[me], len(f_copies), chip, core)
        copy.start()
        f_copies.append(copy)

    for chip in reversed(near):
        both = down_part(chip_lanes(chip))
        for core in range(tp_count):
            send_down(chip, core, both[:, core * cols : (core + 1) * cols])
    for core in beside:
        lanes = pl.ds(pl.multiple_of((kv * tp_count + core) * cols, cols), cols)
        send_down(kv, core, down_part(lanes))
    summed = hid_own + down_part(own_lanes)
    for chip, core in near_peers:
        wait_from(2, frecv, chip, core)
        summed = summed + frecv[chip * tp_count + core].astype(F32)
    own_sum = jnp.sum(summed, 1, keepdims=True)
    own_square = jnp.sum(summed * summed, 1, keepdims=True)
    low_half = lax.broadcasted_iota(jnp.int32, (rows, 128), 1) < 64
    sums[me] = jnp.where(low_half, own_sum, own_square)
    sum_copies = send_all(3, sums)
    for chip, core in near_peers:
        wait_from(3, sums, chip, core)
    all_sums = functools.reduce(lambda a, b: a + b, [sums[p] for p in range(group)])
    mean = all_sums[:, :1] / width
    var = all_sums[:, 64:65] / width - mean * mean
    gain = gout[:, own_lanes]
    out_v[...] = ((summed - mean) * lax.rsqrt(var + 1e-05) * gain).astype(BF16)

    for p in range(4):
        for copy in part_copies(p):
            copy.wait_send()
    for copies in (att_copies, mix_copies, f_copies, sum_copies):
        for copy in copies:
            copy.wait_send()


def store_kernel(out_v, nst_v, out_h, nst_h, sem):
    copies = [
        pltpu.make_async_copy(nst_v, nst_h, sem.at[0]),
        pltpu.make_async_copy(out_v, out_h, sem.at[1]),
    ]
    for copy in copies:
        copy.start()
    for copy in copies:
        copy.wait()


def fused_step(
    tokens,
    positions,
    state,
    w_query,
    w_key,
    w_value,
    w_gate,
    w_out,
    gain_mix,
    w_ffn_gate,
    w_ffn_up,
    w_ffn_down,
    gain_out,
):
    kv_count = lax.axis_size("kv")
    tp_count = lax.axis_size("tp")
    group = kv_count * tp_count
    rows = tokens.shape[0]
    _, heads, width_head, _ = state.shape
    width = w_ffn_gate.shape[0]
    cols = w_out.shape[1]
    half = width_head // 2
    inverse = 10000.0 ** (-np.arange(half, dtype=np.float32) / half)
    inverse = np.tile(inverse.astype(np.float32), 2)[None, :]
    arrays = (
        tokens,
        positions[None, :],
        state[0],
        w_query,
        w_key,
        w_value,
        w_gate,
        w_out,
        gain_mix[None, :],
        w_ffn_gate.T,
        w_ffn_up.T,
        w_ffn_down,
        gain_out[None, :],
        jnp.asarray(inverse),
    )
    held = [pltpu.VMEM(a.shape, a.dtype) for a in arrays]
    held[9:11] = [pltpu.VMEM((2, w_ffn_gate.shape[1], width), BF16)]
    vmem_spec = pl.BlockSpec(memory_space=pltpu.VMEM)
    any_spec = pl.BlockSpec(memory_space=pl.ANY)
    out, new_state = pl.pallas_call(
        functools.partial(step_kernel, kv_count, tp_count),
        out_shape=(
            pltpu.VMEM((rows, cols), BF16),
            pltpu.VMEM(state.shape[1:], F32),
        ),
        in_specs=[any_spec] * len(arrays),
        out_specs=(vmem_spec, vmem_spec),
        scratch_shapes=held
        + [
            pltpu.VMEM((kv_count, 4, heads, width_head), F32),
            pltpu.VMEM((kv_count, 4, heads, width_head), F32),
            pltpu.VMEM((rows, heads * width_head), F32),
            pltpu.VMEM((rows, cols), F32),
            pltpu.VMEM((group, heads, width_head), BF16),
            pltpu.VMEM((group * heads, width_head), F32),
            pltpu.VMEM((group, rows, cols), BF16),
            pltpu.VMEM((8, width), F32),
            pltpu.VMEM((8, w_ffn_gate.shape[1]), F32),
            pltpu.VMEM((8, w_ffn_gate.shape[1]), F32),
            pltpu.VMEM((2 * (kv_count - 1), tp_count * cols, w_ffn_gate.shape[1]), BF16),
            pltpu.VMEM((256, 256), BF16),
            pltpu.VMEM((rows, w_ffn_gate.shape[1]), BF16),
            pltpu.VMEM((group, rows, cols), BF16),
            pltpu.VMEM((group, rows, cols), BF16),
            pltpu.VMEM((group, rows, 128), F32),
        ],
        compiler_params=pltpu.CompilerParams(
            collective_id=0, has_side_effects=True, vmem_limit_bytes=63 * 2**20
        ),
    )(*arrays)
    out, new_state = pl.pallas_call(
        store_kernel,
        out_shape=(
            jax.ShapeDtypeStruct(out.shape, out.dtype),
            jax.ShapeDtypeStruct(new_state.shape, new_state.dtype),
        ),
        in_specs=[vmem_spec, vmem_spec],
        out_specs=(any_spec, any_spec),
        scratch_shapes=[pltpu.SemaphoreType.DMA((2,))],
        compiler_params=pltpu.CompilerParams(vmem_limit_bytes=2**20),
    )(out, new_state)
    return out, new_state[None]


def fits_kernel(tokens, state, w_out, kv_count, tp_count):
    seqs, _, width_head, _ = state.shape
    return (
        seqs == 1
        and width_head == 128
        and w_out.shape[1] % 256 == 0
        and tokens.shape[0] == kv_count
        and 3 <= kv_count <= 6
        and tp_count >= 2
        and kv_count * tp_count <= 16
    )


def rotate(vectors, positions):
    half = vectors.shape[-1] // 2
    inverse = 10000.0 ** (-jnp.arange(half, dtype=jnp.float32) / half)
    angle = positions.astype(jnp.float32)[:, None, None] * inverse[None, None, :]
    cosine = jnp.cos(angle)
    sine = jnp.sin(angle)
    first = vectors[..., :half]
    second = vectors[..., half:]
    return jnp.concatenate([first * cosine - second * sine, first * sine + second * cosine], -1)


def finish_norm(values, sums, squares, count, gain):
    mean = sums / count
    var = squares / count - mean * mean
    return (values - mean[:, None]) * lax.rsqrt(var + 1e-05)[:, None] * gain[None, :]


def on_device(
    tokens,
    positions,
    state,
    w_query,
    w_key,
    w_value,
    w_gate,
    w_out,
    gain_mix,
    w_ffn_gate,
    w_ffn_up,
    w_ffn_down,
    gain_out,
):
    if fits_kernel(tokens, state, w_out, lax.axis_size("kv"), lax.axis_size("tp")):
        return fused_step(
            tokens,
            positions,
            state,
            w_query,
            w_key,
            w_value,
            w_gate,
            w_out,
            gain_mix,
            w_ffn_gate,
            w_ffn_up,
            w_ffn_down,
            gain_out,
        )
    seqs = state.shape[0]
    heads = state.shape[1]
    width_head = state.shape[2]
    proj_cols = w_query.shape[1]
    width = w_ffn_gate.shape[0]
    cols = w_out.shape[1]
    group_rows = tokens.shape[0]
    kv_count = lax.axis_size("kv")
    tp_count = lax.axis_size("tp")
    tp_index = lax.axis_index("tp")
    col_start = (lax.axis_index("kv") * tp_count + tp_index) * cols
    projected = lax.psum_scatter(
        jnp.concatenate(
            [
                jnp.dot(tokens, w_query, preferred_element_type=jnp.float32),
                jnp.dot(tokens, w_key, preferred_element_type=jnp.float32),
                jnp.dot(tokens, w_value, preferred_element_type=jnp.float32),
                jnp.dot(tokens, w_gate, preferred_element_type=jnp.float32),
            ],
            axis=1,
        ),
        "kv",
        scatter_dimension=0,
        tiled=True,
    )
    query = projected[:, :proj_cols].reshape(seqs, heads, width_head)
    key = projected[:, proj_cols : 2 * proj_cols].reshape(seqs, heads, width_head)
    value = projected[:, 2 * proj_cols : 3 * proj_cols].reshape(seqs, heads, width_head)
    gate_pre = projected[:, 3 * proj_cols :]
    query = rotate(query, positions)
    key = rotate(key, positions) * width_head ** (-0.5)
    total_heads = heads * tp_count
    head_ids = (tp_index * heads + jnp.arange(heads, dtype=jnp.int32)).astype(jnp.float32)
    decay = 1.0 - 2.0 ** (-5.0 - 6.0 * head_ids / (total_heads - 1))
    new_state = decay[None, :, None, None] * state + key[:, :, :, None] * value[:, :, None, :]
    retained = jnp.einsum("bhd,bhdv->bhv", query, new_state, precision=lax.Precision.HIGHEST)
    mean = jnp.mean(retained, -1, keepdims=True)
    var = jnp.mean(jnp.square(retained - mean), -1, keepdims=True)
    normed = (retained - mean) * lax.rsqrt(var + 1e-05)
    attended = (normed.reshape(seqs, proj_cols) * jax.nn.silu(gate_pre)).astype(jnp.bfloat16)
    gathered = lax.all_gather(attended[None], ("kv", "tp"), axis=0, tiled=True)
    gathered = gathered.reshape(kv_count, tp_count, seqs, proj_cols)
    out_blocks = w_out.reshape(tp_count, proj_cols, cols)
    mixed = jnp.einsum(
        "itsc,tcd->isd", gathered, out_blocks, preferred_element_type=jnp.float32
    ).reshape(group_rows, cols)
    tokens_own = lax.dynamic_slice_in_dim(tokens, tp_index * cols, cols, 1)
    mixed_pre = (tokens_own.astype(jnp.float32) + mixed).astype(jnp.bfloat16)
    gain_out_own = lax.dynamic_slice_in_dim(gain_out, col_start, cols, 0)
    whole_rows = lax.all_gather(mixed_pre, ("kv", "tp"), axis=1, tiled=True).astype(jnp.float32)
    hidden = finish_norm(
        whole_rows, jnp.sum(whole_rows, 1), jnp.sum(whole_rows * whole_rows, 1), width, gain_mix
    ).astype(jnp.bfloat16)
    hidden_own = lax.dynamic_slice_in_dim(hidden, col_start, cols, 1)
    gate = jnp.dot(hidden, w_ffn_gate, preferred_element_type=jnp.float32)
    upward = jnp.dot(hidden, w_ffn_up, preferred_element_type=jnp.float32)
    inner = (jax.nn.silu(gate) * upward).astype(jnp.bfloat16)
    ffn_cols = lax.psum_scatter(
        lax.dot_general(
            w_ffn_down, inner, (((0,), (1,)), ((), ())), preferred_element_type=jnp.float32
        ),
        ("kv", "tp"),
        scatter_dimension=0,
        tiled=True,
    )
    summed = hidden_own.astype(jnp.float32) + ffn_cols.T
    out_sums, out_squares = lax.psum(
        (jnp.sum(summed, 1), jnp.sum(summed * summed, 1)), ("kv", "tp")
    )
    layer_out = finish_norm(summed, out_sums, out_squares, width, gain_out_own).astype(jnp.bfloat16)
    return (layer_out, new_state)


def solution(mesh):
    return jax.shard_map(
        on_device,
        mesh=mesh,
        in_specs=(
            P("dp", "kv"),
            P(("dp", "kv")),
            P(("dp", "kv"), "tp", None, None),
            P("kv", "tp"),
            P("kv", "tp"),
            P("kv", "tp"),
            P("kv", "tp"),
            P(None, ("kv", "tp")),
            P(),
            P(None, ("kv", "tp")),
            P(None, ("kv", "tp")),
            P(("kv", "tp"), None),
            P(),
        ),
        out_specs=(P("dp", ("kv", "tp")), P(("dp", "kv"), "tp", None, None)),
        check_vma=False,
    )
```

```python
import functools

import jax
import jax.numpy as jnp
import numpy as np
from jax import lax
from jax.experimental import pallas as pl
from jax.experimental.pallas import tpu as pltpu
from jax.sharding import PartitionSpec as P

MESH = pl.DeviceIdType.MESH
F32 = jnp.float32
BF16 = jnp.bfloat16


def dot_rows(values, weight):
    return lax.dot_general(values, weight, (((1,), (1,)), ((), ())), preferred_element_type=F32)


def nearest(kv, count, k):
    low = jnp.minimum(kv, count - 1 - kv)
    step = jnp.where(2 * kv < count, 1, -1)
    side = 1 - 2 * (k % 2)
    return kv + jnp.where(k <= 2 * low, (k + 1) // 2 * side, (k - low) * step)


def step_kernel(kv_count, tp_count, *refs):
    def body(*sems):
        step_body(kv_count, tp_count, *refs, *sems)

    group = kv_count * tp_count
    pl.run_scoped(
        body,
        pltpu.SemaphoreType.DMA((13,)),
        pltpu.SemaphoreType.DMA((kv_count, 2)),
        pltpu.SemaphoreType.DMA((4, kv_count)),
        pltpu.SemaphoreType.DMA((4, kv_count)),
        pltpu.SemaphoreType.DMA((2, tp_count)),
        pltpu.SemaphoreType.DMA((4, group)),
        pltpu.SemaphoreType.DMA((4, group)),
    )


def step_body(
    kv_count,
    tp_count,
    tok_h,
    pos_h,
    state_h,
    wq_h,
    wk_h,
    wv_h,
    wg_h,
    wout_h,
    gmix_h,
    wfg_h,
    wfu_h,
    wfd_h,
    gout_h,
    inv_h,
    out_v,
    nst,
    tok,
    pos,
    state,
    wq,
    wk,
    wv,
    wg,
    wout,
    gmix,
    w_up,
    wfd,
    gout,
    inv,
    qsend,
    qrecv,
    half_part,
    mixed_part,
    gate_recv,
    gates,
    att,
    mix,
    gain_rows,
    acc_gate,
    acc_up,
    turned,
    eye,
    inner,
    fsend,
    frecv,
    sums,
    local_sem,
    up_sem,
    q_send_sem,
    q_recv_sem,
    gate_sem,
    send_sem,
    recv_sem,
):
    group = kv_count * tp_count
    dp = lax.axis_index("dp")
    kv = lax.axis_index("kv")
    tp = lax.axis_index("tp")
    me = kv * tp_count + tp
    rows = tok.shape[0]
    heads = state.shape[0]
    width_head = state.shape[1]
    width = w_up.shape[2]
    cols = mix.shape[2]
    ff = w_up.shape[1]

    near = [nearest(kv, kv_count, k) for k in range(1, kv_count)]
    beside = [lax.rem(tp + e, tp_count) for e in range(1, tp_count)]
    far_peers = [(chip, core) for chip in reversed(near) for core in range(tp_count)]
    near_peers = [(kv, core) for core in beside]
    near_peers += [(chip, core) for chip in near for core in range(tp_count)]

    loads = []

    def load(src, dst):
        copy = pltpu.make_async_copy(src, dst, local_sem.at[len(loads)])
        copy.start()
        loads.append(copy)
        return copy

    tok_load = load(tok_h, tok)
    pos_load = load(pos_h, pos)
    inv_load = load(inv_h, inv)
    deep = wg.shape[0] // 2
    halves = [pl.ds(0, deep), pl.ds(deep, deep)]
    proj_loads = [[load(src, dst)] for src, dst in ((wq_h, wq), (wk_h, wk), (wv_h, wv))]
    proj_loads.append([load(wg_h.at[half], wg.at[half]) for half in halves])
    state_load = load(state_h, state)
    gmix_load = load(gmix_h, gmix)
    gout_load = load(gout_h, gout)

    barrier = pltpu.get_barrier_semaphore()
    for chip, core in far_peers + [(kv, core) for core in beside]:
        pl.semaphore_signal(barrier, inc=1, device_id=(dp, chip, core), device_id_type=MESH)

    pos_load.wait()
    inv_load.wait()
    lane = lax.broadcasted_iota(jnp.int32, (1, width_head), 1)
    eye[...] = jnp.where(
        lax.broadcasted_iota(jnp.int32, eye.shape, 0)
        == lax.broadcasted_iota(jnp.int32, eye.shape, 1),
        1.0,
        0.0,
    ).astype(BF16)
    angle = pos[...].astype(F32) * inv[...]
    cosine = jnp.cos(angle)
    sine = jnp.sin(angle)
    sine = jnp.where(lane < width_head // 2, -sine, sine)

    tok_load.wait()
    later = []

    def part_copies(p):
        return [
            pltpu.make_async_remote_copy(
                src_ref=qsend.at[chip, p] if p < 3 else half_part,
                dst_ref=qrecv.at[kv, p] if p < 3 else gate_recv.at[kv],
                send_sem=q_send_sem.at[p, d],
                recv_sem=q_recv_sem.at[p, kv],
                device_id=(dp, chip, tp),
                device_id_type=MESH,
            )
            for d, chip in reversed(list(enumerate(near)))
        ]

    span = tp_count * cols

    def chip_lanes(chip):
        return pl.ds(pl.multiple_of(chip * span, span), span)

    def up_copy(rank, m):
        chip = nearest(kv, kv_count, kv_count - 1 - rank)
        at = chip_lanes(chip)
        source = (wfg_h, wfu_h)[m] if isinstance(m, int) else wfg_h
        return pltpu.make_async_copy(source.at[:, at], w_up.at[m, :, at], up_sem.at[rank, m])

    stage = jnp.minimum(kv_count - 1 - kv, 3)
    for p, weight in enumerate((wq, wk, wv, wg)):
        proj_loads[p][0].wait()
        if p == 0:
            later.append(load(wout_h, wout))
        ranks = [p] if p < 3 else list(range(3, kv_count))
        for rank in ranks:
            for m in range(2):
                up_copy(rank, m).start()
        if p < 3:
            part = jnp.dot(tok[...], weight[...], preferred_element_type=F32)
        else:
            later.append(load(wfd_h, wfd))
            half_part[...] = jnp.dot(
                tok[:, :deep], weight[:deep], preferred_element_type=F32
            )
            proj_loads[p][1].wait()
            half_part[...] += jnp.dot(
                tok[:, deep:], weight[deep:], preferred_element_type=F32
            )
        for i in range(kv_count if p < 3 else 0):
            for h in range(heads):
                qsend[i, p, h : h + 1, :] = part[
                    i : i + 1, h * width_head : (h + 1) * width_head
                ]

        @pl.when(stage == p)
        def first_sends():
            pl.semaphore_wait(barrier, group - 1)
            for done in range(min(p, 2) + 1):
                for copy in part_copies(done):
                    copy.start()

        if 0 < p < 3:

            @pl.when(stage < p)
            def next_send():
                for copy in part_copies(p):
                    copy.start()

    wout_load, wfd_load = later

    head_id = (tp * heads + lax.broadcasted_iota(jnp.int32, (heads, width_head), 0)).astype(F32)
    total_heads = heads * tp_count
    decay = 1.0 - jnp.exp2(-5.0 - 6.0 * head_id / (total_heads - 1))

    gmix_load.wait()
    gain = gmix[...]
    gain_high = gain.astype(BF16).astype(F32)
    row_id = lax.broadcasted_iota(jnp.int32, (8, width), 0)
    gain_rows[...] = jnp.where(
        row_id == rows, gain_high, jnp.where(row_id == rows + 1, gain - gain_high, 0.0)
    )

    def rotate_row(x):
        return x * cosine + pltpu.roll(x, width_head // 2, 1) * sine

    def collect(p):
        total = qsend[kv, p] if p < 3 else half_part[...]
        for chip in near:
            landed = qrecv.at[chip, p] if p < 3 else gate_recv.at[chip]
            pltpu.make_async_remote_copy(
                src_ref=landed,
                dst_ref=landed,
                send_sem=q_send_sem.at[p, 0],
                recv_sem=q_recv_sem.at[p, chip],
                device_id=(dp, chip, tp),
                device_id_type=MESH,
            ).wait_recv()
            total = total + landed[...]
        return total

    pieces = 2 * (kv_count - 1)

    def by_kv(values):
        return functools.reduce(
            lambda a, b: a + b, [jnp.where(kv == c, n, 0) for c, n in enumerate(values)]
        )

    middle = [pieces // 3] * (kv_count - 2)
    turns = [by_kv([2]), by_kv([pieces - 1] + middle + [1])]
    turns.append(by_kv([pieces] + [n + 2 for n in middle] + [3]))

    def turn(piece, carry):
        rank = piece // 2
        m = piece % 2
        up_copy(rank, m).wait()
        start = nearest(kv, kv_count, kv_count - 1 - rank) * span
        for k in range(0, span, 512):
            for f in range(0, ff, 256):
                n = min(256, ff - f)
                at = pl.ds(pl.multiple_of(start + k, 256), 256)
                turned[piece, k : k + 256, f : f + n] = dot_rows(
                    eye[...], w_up[m, f : f + n, at]
                ).astype(BF16)
                if k + 256 < span:
                    at = pl.ds(pl.multiple_of(start + k + 256, 256), 256)
                    turned[piece, k + 256 : k + 512, f : f + n] = w_up[m, f : f + n, at].T
        return carry

    lax.fori_loop(0, turns[0], turn, 0)
    for copy in part_copies(3):
        copy.start()
    lax.fori_loop(turns[0], turns[1], turn, 0)

    state_load.wait()
    query = rotate_row(collect(0))
    query_t = jnp.transpose(query)
    held = jnp.concatenate(
        [
            jnp.sum(query_t[:, h : h + 1] * state[h], axis=0, keepdims=True)
            for h in range(heads)
        ],
        axis=0,
    )
    key = rotate_row(collect(1)) * width_head ** (-0.5)
    match = jnp.sum(query * key, axis=1, keepdims=True)
    value = collect(2)
    retained = decay * held + match * value
    mean = jnp.mean(retained, -1, keepdims=True)
    var = jnp.mean(jnp.square(retained - mean), -1, keepdims=True)
    normed = (retained - mean) * lax.rsqrt(var + 1e-05)
    att[me] = normed

    def remote(phase, src, dst, slot, chip, core):
        return pltpu.make_async_remote_copy(
            src_ref=src,
            dst_ref=dst,
            send_sem=send_sem.at[phase, slot],
            recv_sem=recv_sem.at[phase, me],
            device_id=(dp, chip, core),
            device_id_type=MESH,
        )

    def send_all(phase, ref):
        copies = []
        for chip, core in far_peers + [(kv, core) for core in beside]:
            copy = remote(phase, ref.at[me], ref.at[me], len(copies), chip, core)
            copy.start()
            copies.append(copy)
        return copies

    def wait_from(phase, ref, chip, core):
        source = chip * tp_count + core
        pltpu.make_async_remote_copy(
            src_ref=ref.at[me],
            dst_ref=ref.at[source],
            send_sem=send_sem.at[phase, 0],
            recv_sem=recv_sem.at[phase, source],
            device_id=(dp, chip, core),
            device_id_type=MESH,
        ).wait_recv()

    att_copies = send_all(0, att)

    lax.fori_loop(turns[1], turns[2], turn, 0)

    gate_pre = collect(3)
    gates[tp] = gate_pre / (1.0 + jnp.exp(-gate_pre))

    def gate_copy(core):
        return pltpu.make_async_remote_copy(
            src_ref=gates.at[tp],
            dst_ref=gates.at[tp],
            send_sem=gate_sem.at[0, core],
            recv_sem=gate_sem.at[1, tp],
            device_id=(dp, kv, core),
            device_id_type=MESH,
        )

    for core in beside:
        gate_copy(core).start()

    key_t = jnp.transpose(key)
    for h in range(heads):
        nst[h] = decay[h : h + 1, :] * state[h] + key_t[:, h : h + 1] * value[h : h + 1, :]

    lax.fori_loop(turns[2], pieces, turn, 0)

    wout_load.wait()
    mixed = None
    for t in reversed(range(tp_count)):
        for chip in near:
            wait_from(0, att, chip, t)

        @pl.when(tp != t)
        def wait_beside():
            wait_from(0, att, kv, t)
            pltpu.make_async_remote_copy(
                src_ref=gates.at[t],
                dst_ref=gates.at[t],
                send_sem=gate_sem.at[0, t],
                recv_sem=gate_sem.at[1, t],
                device_id=(dp, kv, t),
                device_id_type=MESH,
            ).wait_recv()

        lhs = jnp.concatenate(
            [att[pl.ds(t, rows, stride=tp_count), h, :] for h in range(heads)], axis=1
        )
        lhs = (lhs * gates[t]).astype(BF16)
        depth = heads * width_head
        part = jnp.dot(lhs, wout[t * depth : (t + 1) * depth], preferred_element_type=F32)
        if t > 0:
            if t < tp_count - 1:
                part = part + mixed_part[...]
            mixed_part[...] = part
        else:
            mixed = part + mixed_part[...]
    tok_own = tok[:, pl.ds(pl.multiple_of(tp * cols, cols), cols)]
    own = (tok_own.astype(F32) + mixed).astype(BF16)
    mix[me] = own
    mix_copies = send_all(1, mix)

    own = own.astype(F32)
    shift = jnp.mean(own, 1, keepdims=True)
    gout_load.wait()
    for m in range(2):
        up_copy(kv_count - 1, m).wait()
    tile = 256
    starts = list(range(0, ff, tile))
    own_lanes = pl.ds(pl.multiple_of(me * cols, cols), cols)

    def centred(x, lanes):
        z = jnp.concatenate([x * gmix[:, lanes], jnp.zeros((8 - rows, x.shape[1]), F32)], 0)
        return (z + gain_rows[:, lanes]).astype(BF16)

    def up_turned(lhs, rank):
        for start in starts:
            at = pl.ds(start, min(tile, ff - start))
            for m, acc in enumerate((acc_gate, acc_up)):
                acc[:, at] += jnp.dot(
                    lhs, turned[2 * rank + m, :, at], preferred_element_type=F32
                )

    def up_part(lhs, lanes, first):
        for start in starts:
            at = pl.ds(start, min(tile, ff - start))
            for m, acc in enumerate((acc_gate, acc_up)):
                part = dot_rows(lhs, w_up[m, at, lanes])
                acc[:, at] = part if first else acc[:, at] + part

    own = own - shift
    up_part(centred(own, own_lanes), own_lanes, True)
    total = own
    squares = own * own
    for core in beside:
        wait_from(1, mix, kv, core)
        lanes = pl.ds(pl.multiple_of((kv * tp_count + core) * cols, cols), cols)
        x = mix[kv * tp_count + core].astype(F32) - shift
        total = total + x
        squares = squares + x * x
        up_part(centred(x, lanes), lanes, False)
    for k, chip in enumerate(near):
        for core in range(tp_count):
            wait_from(1, mix, chip, core)
        if k == kv_count - 2:
            wfd_load.wait()
        blocks = []
        for core in range(tp_count):
            lanes = pl.ds(pl.multiple_of((chip * tp_count + core) * cols, cols), cols)
            x = mix[chip * tp_count + core].astype(F32) - shift
            total = total + x
            squares = squares + x * x
            blocks.append(centred(x, lanes))
        up_turned(jnp.concatenate(blocks, 1), kv_count - 2 - k)

    mean = jnp.sum(total, 1, keepdims=True) / width
    var = jnp.sum(squares, 1, keepdims=True) / width - mean * mean
    scale = lax.rsqrt(var + 1e-05)
    hid_own = ((own - mean) * scale * gmix[:, own_lanes]).astype(BF16).astype(F32)

    def finish(acc, at):
        bias = acc[rows : rows + 1, at] + acc[rows + 1 : rows + 2, at]
        return scale * (acc[:rows, at] - mean * bias)

    for start in starts:
        at = pl.ds(start, min(tile, ff - start))
        gate = finish(acc_gate, at)
        inner[:, at] = (gate / (1.0 + jnp.exp(-gate)) * finish(acc_up, at)).astype(BF16)

    main = ff // 128 * 128

    def down_part(at):
        result = jnp.dot(inner[:, :main], wfd[:main, at], preferred_element_type=F32)
        if main < ff:
            result += jnp.dot(inner[:, main:], wfd[main:, at], preferred_element_type=F32)
        return result

    f_copies = []

    def send_down(chip, core, result):
        owner = chip * tp_count + core
        fsend[owner] = result.astype(BF16)
        copy = remote(2, fsend.at[owner], frecv.at[me], len(f_copies), chip, core)
        copy.start()
        f_copies.append(copy)

    for chip in reversed(near):
        both = down_part(chip_lanes(chip))
        for core in range(tp_count):
            send_down(chip, core, both[:, core * cols : (core + 1) * cols])
    for core in beside:
        lanes = pl.ds(pl.multiple_of((kv * tp_count + core) * cols, cols), cols)
        send_down(kv, core, down_part(lanes))
    summed = hid_own + down_part(own_lanes)
    for chip, core in near_peers:
        wait_from(2, frecv, chip, core)
        summed = summed + frecv[chip * tp_count + core].astype(F32)
    own_sum = jnp.sum(summed, 1, keepdims=True)
    own_square = jnp.sum(summed * summed, 1, keepdims=True)
    own_sums = [jnp.broadcast_to(x, (rows, 128)) for x in (own_sum, own_square)]
    sums[me] = jnp.concatenate(own_sums, 1)
    sum_copies = send_all(3, sums)
    for p in range(4):
        for copy in part_copies(p):
            copy.wait_send()
    for core in beside:
        gate_copy(core).wait_send()
    for copies in (att_copies, mix_copies, f_copies):
        for copy in copies:
            copy.wait_send()
    for chip, core in near_peers:
        wait_from(3, sums, chip, core)
    all_sums = functools.reduce(lambda a, b: a + b, [sums[p] for p in range(group)])
    mean = all_sums[:, :128] / width
    var = all_sums[:, 128:] / width - mean * mean
    scale = lax.rsqrt(var + 1e-05)
    mean, scale = [jnp.concatenate([x] * (cols // 128), 1) for x in (mean, scale)]
    out_v[...] = ((summed - mean) * scale * gout[:, own_lanes]).astype(BF16)

    for copy in sum_copies:
        copy.wait_send()


def store_kernel(out_v, nst_v, out_h, nst_h, sem):
    copies = [
        pltpu.make_async_copy(nst_v, nst_h, sem.at[0]),
        pltpu.make_async_copy(out_v, out_h, sem.at[1]),
    ]
    for copy in copies:
        copy.start()
    for copy in copies:
        copy.wait()


def fused_step(
    tokens,
    positions,
    state,
    w_query,
    w_key,
    w_value,
    w_gate,
    w_out,
    gain_mix,
    w_ffn_gate,
    w_ffn_up,
    w_ffn_down,
    gain_out,
):
    kv_count = lax.axis_size("kv")
    tp_count = lax.axis_size("tp")
    group = kv_count * tp_count
    rows = tokens.shape[0]
    _, heads, width_head, _ = state.shape
    width = w_ffn_gate.shape[0]
    cols = w_out.shape[1]
    half = width_head // 2
    inverse = 10000.0 ** (-np.arange(half, dtype=np.float32) / half)
    inverse = np.tile(inverse.astype(np.float32), 2)[None, :]
    arrays = (
        tokens,
        positions[None, :],
        state[0],
        w_query,
        w_key,
        w_value,
        w_gate,
        w_out,
        gain_mix[None, :],
        w_ffn_gate.T,
        w_ffn_up.T,
        w_ffn_down,
        gain_out[None, :],
        jnp.asarray(inverse),
    )
    held = [pltpu.VMEM(a.shape, a.dtype) for a in arrays]
    held[9:11] = [pltpu.VMEM((2, w_ffn_gate.shape[1], width), BF16)]
    vmem_spec = pl.BlockSpec(memory_space=pltpu.VMEM)
    any_spec = pl.BlockSpec(memory_space=pl.ANY)
    out, new_state = pl.pallas_call(
        functools.partial(step_kernel, kv_count, tp_count),
        out_shape=(
            pltpu.VMEM((rows, cols), BF16),
            pltpu.VMEM(state.shape[1:], F32),
        ),
        in_specs=[any_spec] * len(arrays),
        out_specs=(vmem_spec, vmem_spec),
        scratch_shapes=held
        + [
            pltpu.VMEM((kv_count, 3, heads, width_head), F32),
            pltpu.VMEM((kv_count, 3, heads, width_head), F32),
            pltpu.VMEM((rows, heads * width_head), F32),
            pltpu.VMEM((rows, cols), F32),
            pltpu.VMEM((kv_count, rows, heads * width_head), F32),
            pltpu.VMEM((tp_count, rows, heads * width_head), F32),
            pltpu.VMEM((group, heads, width_head), F32),
            pltpu.VMEM((group, rows, cols), BF16),
            pltpu.VMEM((8, width), F32),
            pltpu.VMEM((8, w_ffn_gate.shape[1]), F32),
            pltpu.VMEM((8, w_ffn_gate.shape[1]), F32),
            pltpu.VMEM((2 * (kv_count - 1), tp_count * cols, w_ffn_gate.shape[1]), BF16),
            pltpu.VMEM((256, 256), BF16),
            pltpu.VMEM((rows, w_ffn_gate.shape[1]), BF16),
            pltpu.VMEM((group, rows, cols), BF16),
            pltpu.VMEM((group, rows, cols), BF16),
            pltpu.VMEM((group, rows, 256), F32),
        ],
        compiler_params=pltpu.CompilerParams(
            collective_id=0, has_side_effects=True, vmem_limit_bytes=63 * 2**20
        ),
    )(*arrays)
    out, new_state = pl.pallas_call(
        store_kernel,
        out_shape=(
            jax.ShapeDtypeStruct(out.shape, out.dtype),
            jax.ShapeDtypeStruct(new_state.shape, new_state.dtype),
        ),
        in_specs=[vmem_spec, vmem_spec],
        out_specs=(any_spec, any_spec),
        scratch_shapes=[pltpu.SemaphoreType.DMA((2,))],
        compiler_params=pltpu.CompilerParams(vmem_limit_bytes=2**20),
    )(out, new_state)
    return out, new_state[None]


def fits_kernel(tokens, state, w_out, kv_count, tp_count):
    seqs, _, width_head, _ = state.shape
    return (
        seqs == 1
        and width_head == 128
        and w_out.shape[1] % 256 == 0
        and tokens.shape[0] == kv_count
        and 3 <= kv_count <= 6
        and tp_count >= 2
        and kv_count * tp_count <= 16
    )


def rotate(vectors, positions):
    half = vectors.shape[-1] // 2
    inverse = 10000.0 ** (-jnp.arange(half, dtype=jnp.float32) / half)
    angle = positions.astype(jnp.float32)[:, None, None] * inverse[None, None, :]
    cosine = jnp.cos(angle)
    sine = jnp.sin(angle)
    first = vectors[..., :half]
    second = vectors[..., half:]
    return jnp.concatenate([first * cosine - second * sine, first * sine + second * cosine], -1)


def finish_norm(values, sums, squares, count, gain):
    mean = sums / count
    var = squares / count - mean * mean
    return (values - mean[:, None]) * lax.rsqrt(var + 1e-05)[:, None] * gain[None, :]


def on_device(
    tokens,
    positions,
    state,
    w_query,
    w_key,
    w_value,
    w_gate,
    w_out,
    gain_mix,
    w_ffn_gate,
    w_ffn_up,
    w_ffn_down,
    gain_out,
):
    if fits_kernel(tokens, state, w_out, lax.axis_size("kv"), lax.axis_size("tp")):
        return fused_step(
            tokens,
            positions,
            state,
            w_query,
            w_key,
            w_value,
            w_gate,
            w_out,
            gain_mix,
            w_ffn_gate,
            w_ffn_up,
            w_ffn_down,
            gain_out,
        )
    seqs = state.shape[0]
    heads = state.shape[1]
    width_head = state.shape[2]
    proj_cols = w_query.shape[1]
    width = w_ffn_gate.shape[0]
    cols = w_out.shape[1]
    group_rows = tokens.shape[0]
    kv_count = lax.axis_size("kv")
    tp_count = lax.axis_size("tp")
    tp_index = lax.axis_index("tp")
    col_start = (lax.axis_index("kv") * tp_count + tp_index) * cols
    projected = lax.psum_scatter(
        jnp.concatenate(
            [
                jnp.dot(tokens, w_query, preferred_element_type=jnp.float32),
                jnp.dot(tokens, w_key, preferred_element_type=jnp.float32),
                jnp.dot(tokens, w_value, preferred_element_type=jnp.float32),
                jnp.dot(tokens, w_gate, preferred_element_type=jnp.float32),
            ],
            axis=1,
        ),
        "kv",
        scatter_dimension=0,
        tiled=True,
    )
    query = projected[:, :proj_cols].reshape(seqs, heads, width_head)
    key = projected[:, proj_cols : 2 * proj_cols].reshape(seqs, heads, width_head)
    value = projected[:, 2 * proj_cols : 3 * proj_cols].reshape(seqs, heads, width_head)
    gate_pre = projected[:, 3 * proj_cols :]
    query = rotate(query, positions)
    key = rotate(key, positions) * width_head ** (-0.5)
    total_heads = heads * tp_count
    head_ids = (tp_index * heads + jnp.arange(heads, dtype=jnp.int32)).astype(jnp.float32)
    decay = 1.0 - 2.0 ** (-5.0 - 6.0 * head_ids / (total_heads - 1))
    new_state = decay[None, :, None, None] * state + key[:, :, :, None] * value[:, :, None, :]
    retained = jnp.einsum("bhd,bhdv->bhv", query, new_state, precision=lax.Precision.HIGHEST)
    mean = jnp.mean(retained, -1, keepdims=True)
    var = jnp.mean(jnp.square(retained - mean), -1, keepdims=True)
    normed = (retained - mean) * lax.rsqrt(var + 1e-05)
    attended = (normed.reshape(seqs, proj_cols) * jax.nn.silu(gate_pre)).astype(jnp.bfloat16)
    gathered = lax.all_gather(attended[None], ("kv", "tp"), axis=0, tiled=True)
    gathered = gathered.reshape(kv_count, tp_count, seqs, proj_cols)
    out_blocks = w_out.reshape(tp_count, proj_cols, cols)
    mixed = jnp.einsum(
        "itsc,tcd->isd", gathered, out_blocks, preferred_element_type=jnp.float32
    ).reshape(group_rows, cols)
    tokens_own = lax.dynamic_slice_in_dim(tokens, tp_index * cols, cols, 1)
    mixed_pre = (tokens_own.astype(jnp.float32) + mixed).astype(jnp.bfloat16)
    gain_out_own = lax.dynamic_slice_in_dim(gain_out, col_start, cols, 0)
    whole_rows = lax.all_gather(mixed_pre, ("kv", "tp"), axis=1, tiled=True).astype(jnp.float32)
    hidden = finish_norm(
        whole_rows, jnp.sum(whole_rows, 1), jnp.sum(whole_rows * whole_rows, 1), width, gain_mix
    ).astype(jnp.bfloat16)
    hidden_own = lax.dynamic_slice_in_dim(hidden, col_start, cols, 1)
    gate = jnp.dot(hidden, w_ffn_gate, preferred_element_type=jnp.float32)
    upward = jnp.dot(hidden, w_ffn_up, preferred_element_type=jnp.float32)
    inner = (jax.nn.silu(gate) * upward).astype(jnp.bfloat16)
    ffn_cols = lax.psum_scatter(
        lax.dot_general(
            w_ffn_down, inner, (((0,), (1,)), ((), ())), preferred_element_type=jnp.float32
        ),
        ("kv", "tp"),
        scatter_dimension=0,
        tiled=True,
    )
    summed = hidden_own.astype(jnp.float32) + ffn_cols.T
    out_sums, out_squares = lax.psum(
        (jnp.sum(summed, 1), jnp.sum(summed * summed, 1)), ("kv", "tp")
    )
    layer_out = finish_norm(summed, out_sums, out_squares, width, gain_out_own).astype(jnp.bfloat16)
    return (layer_out, new_state)


def solution(mesh):
    return jax.shard_map(
        on_device,
        mesh=mesh,
        in_specs=(
            P("dp", "kv"),
            P(("dp", "kv")),
            P(("dp", "kv"), "tp", None, None),
            P("kv", "tp"),
            P("kv", "tp"),
            P("kv", "tp"),
            P("kv", "tp"),
            P(None, ("kv", "tp")),
            P(),
            P(None, ("kv", "tp")),
            P(None, ("kv", "tp")),
            P(("kv", "tp"), None),
            P(),
        ),
        out_specs=(P("dp", ("kv", "tp")), P(("dp", "kv"), "tp", None, None)),
        check_vma=False,
    )
```

```python
import functools

import jax
import jax.numpy as jnp
import numpy as np
from jax import lax
from jax.experimental import pallas as pl
from jax.experimental.pallas import tpu as pltpu
from jax.sharding import PartitionSpec as P

MESH = pl.DeviceIdType.MESH
F32 = jnp.float32
BF16 = jnp.bfloat16


def dot_rows(values, weight):
    return lax.dot_general(values, weight, (((1,), (1,)), ((), ())), preferred_element_type=F32)


def nearest(kv, count, k):
    low = jnp.minimum(kv, count - 1 - kv)
    step = jnp.where(2 * kv < count, 1, -1)
    side = 1 - 2 * (k % 2)
    return kv + jnp.where(k <= 2 * low, (k + 1) // 2 * side, (k - low) * step)


def step_kernel(kv_count, tp_count, *refs):
    def body(*sems):
        step_body(kv_count, tp_count, *refs, *sems)

    group = kv_count * tp_count
    pl.run_scoped(
        body,
        pltpu.SemaphoreType.DMA((13,)),
        pltpu.SemaphoreType.DMA((kv_count, 2)),
        pltpu.SemaphoreType.DMA((4, kv_count)),
        pltpu.SemaphoreType.DMA((4, kv_count)),
        pltpu.SemaphoreType.DMA((2, tp_count)),
        pltpu.SemaphoreType.DMA((4, group)),
        pltpu.SemaphoreType.DMA((4, group)),
    )


def step_body(
    kv_count,
    tp_count,
    tok_h,
    pos_h,
    state_h,
    wq_h,
    wk_h,
    wv_h,
    wg_h,
    wout_h,
    gmix_h,
    wfg_h,
    wfu_h,
    wfd_h,
    gout_h,
    inv_h,
    out_v,
    nst,
    tok,
    pos,
    state,
    wq,
    wk,
    wv,
    wg,
    wout,
    gmix,
    w_up,
    wfd,
    gout,
    inv,
    qsend,
    qrecv,
    half_part,
    mixed_part,
    gate_recv,
    gates,
    att,
    mix,
    gain_rows,
    acc_gate,
    acc_up,
    turned,
    eye,
    inner,
    fsend,
    frecv,
    sums,
    local_sem,
    up_sem,
    q_send_sem,
    q_recv_sem,
    gate_sem,
    send_sem,
    recv_sem,
):
    group = kv_count * tp_count
    dp = lax.axis_index("dp")
    kv = lax.axis_index("kv")
    tp = lax.axis_index("tp")
    me = kv * tp_count + tp
    rows = tok.shape[0]
    heads = state.shape[0]
    width_head = state.shape[1]
    width = w_up.shape[2]
    cols = mix.shape[2]
    ff = w_up.shape[1]

    near = [nearest(kv, kv_count, k) for k in range(1, kv_count)]
    beside = [lax.rem(tp + e, tp_count) for e in range(1, tp_count)]
    far_peers = [(chip, core) for chip in reversed(near) for core in range(tp_count)]
    near_peers = [(kv, core) for core in beside]
    near_peers += [(chip, core) for chip in near for core in range(tp_count)]

    loads = []

    def load(src, dst):
        copy = pltpu.make_async_copy(src, dst, local_sem.at[len(loads)])
        copy.start()
        loads.append(copy)
        return copy

    tok_load = load(tok_h, tok)
    pos_load = load(pos_h, pos)
    inv_load = load(inv_h, inv)
    deep = wg.shape[0] // 2
    halves = [pl.ds(0, deep), pl.ds(deep, deep)]
    proj_loads = [[load(src, dst)] for src, dst in ((wq_h, wq), (wk_h, wk), (wv_h, wv))]
    proj_loads.append([load(wg_h.at[half], wg.at[half]) for half in halves])
    state_load = load(state_h, state)
    gmix_load = load(gmix_h, gmix)
    gout_load = load(gout_h, gout)

    barrier = pltpu.get_barrier_semaphore()
    for chip, core in far_peers + [(kv, core) for core in beside]:
        pl.semaphore_signal(barrier, inc=1, device_id=(dp, chip, core), device_id_type=MESH)

    pos_load.wait()
    inv_load.wait()
    lane = lax.broadcasted_iota(jnp.int32, (1, width_head), 1)
    eye[...] = jnp.where(
        lax.broadcasted_iota(jnp.int32, eye.shape, 0)
        == lax.broadcasted_iota(jnp.int32, eye.shape, 1),
        1.0,
        0.0,
    ).astype(BF16)
    angle = pos[...].astype(F32) * inv[...]
    cosine = jnp.cos(angle)
    sine = jnp.sin(angle)
    sine = jnp.where(lane < width_head // 2, -sine, sine)

    tok_load.wait()
    later = []

    def part_copies(p):
        return [
            pltpu.make_async_remote_copy(
                src_ref=qsend.at[chip, p] if p < 3 else half_part,
                dst_ref=qrecv.at[kv, p] if p < 3 else gate_recv.at[kv],
                send_sem=q_send_sem.at[p, d],
                recv_sem=q_recv_sem.at[p, kv],
                device_id=(dp, chip, tp),
                device_id_type=MESH,
            )
            for d, chip in reversed(list(enumerate(near)))
        ]

    span = tp_count * cols

    def chip_lanes(chip):
        return pl.ds(pl.multiple_of(chip * span, span), span)

    def up_copy(rank, m):
        chip = nearest(kv, kv_count, kv_count - 1 - rank)
        at = chip_lanes(chip)
        source = (wfg_h, wfu_h)[m] if isinstance(m, int) else wfg_h
        return pltpu.make_async_copy(source.at[:, at], w_up.at[m, :, at], up_sem.at[rank, m])

    stage = jnp.minimum(kv_count - 1 - kv, 3)
    for p, weight in enumerate((wq, wk, wv, wg)):
        proj_loads[p][0].wait()
        if p == 0:
            later.append(load(wout_h, wout))
        ranks = [p] if p < 3 else list(range(3, kv_count))
        for rank in ranks:
            for m in range(2):
                up_copy(rank, m).start()
        if p < 3:
            part = jnp.dot(tok[...], weight[...], preferred_element_type=F32)
        else:
            later.append(load(wfd_h, wfd))
            half_part[...] = jnp.dot(
                tok[:, :deep], weight[:deep], preferred_element_type=F32
            )
            proj_loads[p][1].wait()
            half_part[...] += jnp.dot(
                tok[:, deep:], weight[deep:], preferred_element_type=F32
            )
        for i in range(kv_count if p < 3 else 0):
            for h in range(heads):
                qsend[i, p, h : h + 1, :] = part[
                    i : i + 1, h * width_head : (h + 1) * width_head
                ]

        @pl.when(stage == p)
        def first_sends():
            pl.semaphore_wait(barrier, group - 1)
            for done in range(min(p, 2) + 1):
                for copy in part_copies(done):
                    copy.start()

        if 0 < p < 3:

            @pl.when(stage < p)
            def next_send():
                for copy in part_copies(p):
                    copy.start()

    wout_load, wfd_load = later

    head_id = (tp * heads + lax.broadcasted_iota(jnp.int32, (heads, width_head), 0)).astype(F32)
    total_heads = heads * tp_count
    decay = 1.0 - jnp.exp2(-5.0 - 6.0 * head_id / (total_heads - 1))

    gmix_load.wait()
    gain = gmix[...]
    gain_high = gain.astype(BF16).astype(F32)
    row_id = lax.broadcasted_iota(jnp.int32, (8, width), 0)
    gain_rows[...] = jnp.where(
        row_id == rows, gain_high, jnp.where(row_id == rows + 1, gain - gain_high, 0.0)
    )

    def rotate_row(x):
        return x * cosine + pltpu.roll(x, width_head // 2, 1) * sine

    def collect(p):
        total = qsend[kv, p] if p < 3 else half_part[...]
        for chip in near:
            landed = qrecv.at[chip, p] if p < 3 else gate_recv.at[chip]
            pltpu.make_async_remote_copy(
                src_ref=landed,
                dst_ref=landed,
                send_sem=q_send_sem.at[p, 0],
                recv_sem=q_recv_sem.at[p, chip],
                device_id=(dp, chip, tp),
                device_id_type=MESH,
            ).wait_recv()
            total = total + landed[...]
        return total

    pieces = 2 * (kv_count - 1)

    def by_kv(values):
        return functools.reduce(
            lambda a, b: a + b, [jnp.where(kv == c, n, 0) for c, n in enumerate(values)]
        )

    middle = [pieces // 3] * (kv_count - 2)
    turns = [by_kv([2]), by_kv([pieces - 1] + middle + [1])]
    turns.append(by_kv([pieces] + [n + 2 for n in middle] + [3]))

    def turn(piece, carry):
        rank = piece // 2
        m = piece % 2
        up_copy(rank, m).wait()
        start = nearest(kv, kv_count, kv_count - 1 - rank) * span
        for k in range(0, span, 512):
            for f in range(0, ff, 256):
                n = min(256, ff - f)
                at = pl.ds(pl.multiple_of(start + k, 256), 256)
                turned[piece, k : k + 256, f : f + n] = dot_rows(
                    eye[...], w_up[m, f : f + n, at]
                ).astype(BF16)
                if k + 256 < span:
                    at = pl.ds(pl.multiple_of(start + k + 256, 256), 256)
                    turned[piece, k + 256 : k + 512, f : f + n] = w_up[m, f : f + n, at].T
        return carry

    lax.fori_loop(0, turns[0], turn, 0)
    for copy in part_copies(3):
        copy.start()
    lax.fori_loop(turns[0], turns[1], turn, 0)

    state_load.wait()
    query = rotate_row(collect(0))
    query_t = jnp.transpose(query)
    held = jnp.concatenate(
        [
            jnp.sum(query_t[:, h : h + 1] * state[h], axis=0, keepdims=True)
            for h in range(heads)
        ],
        axis=0,
    )
    key = rotate_row(collect(1)) * width_head ** (-0.5)
    match = jnp.sum(query * key, axis=1, keepdims=True)
    value = collect(2)
    retained = decay * held + match * value
    mean = jnp.mean(retained, -1, keepdims=True)
    var = jnp.mean(jnp.square(retained - mean), -1, keepdims=True)
    normed = (retained - mean) * lax.rsqrt(var + 1e-05)
    att[me] = normed

    def remote(phase, src, dst, slot, chip, core):
        return pltpu.make_async_remote_copy(
            src_ref=src,
            dst_ref=dst,
            send_sem=send_sem.at[phase, slot],
            recv_sem=recv_sem.at[phase, me],
            device_id=(dp, chip, core),
            device_id_type=MESH,
        )

    def send_all(phase, ref):
        copies = []
        for chip, core in far_peers + [(kv, core) for core in beside]:
            copy = remote(phase, ref.at[me], ref.at[me], len(copies), chip, core)
            copy.start()
            copies.append(copy)
        return copies

    def wait_from(phase, ref, chip, core):
        source = chip * tp_count + core
        pltpu.make_async_remote_copy(
            src_ref=ref.at[me],
            dst_ref=ref.at[source],
            send_sem=send_sem.at[phase, 0],
            recv_sem=recv_sem.at[phase, source],
            device_id=(dp, chip, core),
            device_id_type=MESH,
        ).wait_recv()

    att_copies = send_all(0, att)

    lax.fori_loop(turns[1], turns[2], turn, 0)

    gate_pre = collect(3)
    gates[tp] = gate_pre / (1.0 + jnp.exp(-gate_pre))

    def gate_copy(core):
        return pltpu.make_async_remote_copy(
            src_ref=gates.at[tp],
            dst_ref=gates.at[tp],
            send_sem=gate_sem.at[0, core],
            recv_sem=gate_sem.at[1, tp],
            device_id=(dp, kv, core),
            device_id_type=MESH,
        )

    for core in beside:
        gate_copy(core).start()

    key_t = jnp.transpose(key)
    for h in range(heads):
        nst[h] = decay[h : h + 1, :] * state[h] + key_t[:, h : h + 1] * value[h : h + 1, :]

    lax.fori_loop(turns[2], pieces, turn, 0)

    wout_load.wait()
    mixed = None
    for t in reversed(range(tp_count)):
        for chip in near:
            wait_from(0, att, chip, t)

        @pl.when(tp != t)
        def wait_beside():
            wait_from(0, att, kv, t)
            pltpu.make_async_remote_copy(
                src_ref=gates.at[t],
                dst_ref=gates.at[t],
                send_sem=gate_sem.at[0, t],
                recv_sem=gate_sem.at[1, t],
                device_id=(dp, kv, t),
                device_id_type=MESH,
            ).wait_recv()

        lhs = jnp.concatenate(
            [att[pl.ds(t, rows, stride=tp_count), h, :] for h in range(heads)], axis=1
        )
        lhs = (lhs * gates[t]).astype(BF16)
        depth = heads * width_head
        part = jnp.dot(lhs, wout[t * depth : (t + 1) * depth], preferred_element_type=F32)
        if t > 0:
            if t < tp_count - 1:
                part = part + mixed_part[...]
            mixed_part[...] = part
        else:
            mixed = part + mixed_part[...]
    tok_own = tok[:, pl.ds(pl.multiple_of(tp * cols, cols), cols)]
    own = (tok_own.astype(F32) + mixed).astype(BF16)
    mix[me] = own
    mix_copies = send_all(1, mix)

    own = own.astype(F32)
    shift = jnp.mean(own, 1, keepdims=True)
    gout_load.wait()
    for m in range(2):
        up_copy(kv_count - 1, m).wait()
    tile = 256
    starts = list(range(0, ff, tile))
    own_lanes = pl.ds(pl.multiple_of(me * cols, cols), cols)

    def centred(x, lanes):
        z = jnp.concatenate([x * gmix[:, lanes], jnp.zeros((8 - rows, x.shape[1]), F32)], 0)
        return (z + gain_rows[:, lanes]).astype(BF16)

    def up_turned(lhs, rank, depth):
        for start in starts:
            at = pl.ds(start, min(tile, ff - start))
            for m, acc in enumerate((acc_gate, acc_up)):
                acc[:, at] += jnp.dot(
                    lhs, turned[2 * rank + m, depth, at], preferred_element_type=F32
                )

    def up_part(lhs, lanes, first):
        for start in starts:
            at = pl.ds(start, min(tile, ff - start))
            for m, acc in enumerate((acc_gate, acc_up)):
                part = dot_rows(lhs, w_up[m, at, lanes])
                acc[:, at] = part if first else acc[:, at] + part

    own = own - shift
    up_part(centred(own, own_lanes), own_lanes, True)
    total = own
    squares = own * own
    for core in beside:
        wait_from(1, mix, kv, core)
        lanes = pl.ds(pl.multiple_of((kv * tp_count + core) * cols, cols), cols)
        x = mix[kv * tp_count + core].astype(F32) - shift
        total = total + x
        squares = squares + x * x
        up_part(centred(x, lanes), lanes, False)
    for k, chip in enumerate(near):
        order = list(reversed(range(tp_count)))
        if k == kv_count - 2:
            wfd_load.wait()
        for part in [[core] for core in order] if k in (0,) else [order]:
            for core in part:
                wait_from(1, mix, chip, core)
            blocks = []
            for core in sorted(part):
                lanes = pl.ds(pl.multiple_of((chip * tp_count + core) * cols, cols), cols)
                x = mix[chip * tp_count + core].astype(F32) - shift
                total = total + x
                squares = squares + x * x
                blocks.append(centred(x, lanes))
            depth = pl.ds(min(part) * cols, len(part) * cols)
            up_turned(jnp.concatenate(blocks, 1), kv_count - 2 - k, depth)

    mean = jnp.sum(total, 1, keepdims=True) / width
    var = jnp.sum(squares, 1, keepdims=True) / width - mean * mean
    scale = lax.rsqrt(var + 1e-05)
    hid_own = ((own - mean) * scale * gmix[:, own_lanes]).astype(BF16).astype(F32)

    def finish(acc, at):
        bias = acc[rows : rows + 1, at] + acc[rows + 1 : rows + 2, at]
        return scale * (acc[:rows, at] - mean * bias)

    for start in starts:
        at = pl.ds(start, min(tile, ff - start))
        gate = finish(acc_gate, at)
        inner[:, at] = (gate / (1.0 + jnp.exp(-gate)) * finish(acc_up, at)).astype(BF16)

    main = ff // 128 * 128

    def down_part(at):
        result = jnp.dot(inner[:, :main], wfd[:main, at], preferred_element_type=F32)
        if main < ff:
            result += jnp.dot(inner[:, main:], wfd[main:, at], preferred_element_type=F32)
        return result

    f_copies = []

    def send_down(chip, core, result):
        owner = chip * tp_count + core
        fsend[owner] = result.astype(BF16)
        copy = remote(2, fsend.at[owner], frecv.at[me], len(f_copies), chip, core)
        copy.start()
        f_copies.append(copy)

    for chip in reversed(near):
        both = down_part(chip_lanes(chip))
        for core in range(tp_count):
            send_down(chip, core, both[:, core * cols : (core + 1) * cols])
    for core in beside:
        lanes = pl.ds(pl.multiple_of((kv * tp_count + core) * cols, cols), cols)
        send_down(kv, core, down_part(lanes))
    summed = hid_own + down_part(own_lanes)
    for chip, core in near_peers:
        wait_from(2, frecv, chip, core)
        summed = summed + frecv[chip * tp_count + core].astype(F32)
    own_sum = jnp.sum(summed, 1, keepdims=True)
    own_square = jnp.sum(summed * summed, 1, keepdims=True)
    own_sums = [jnp.broadcast_to(x, (rows, 128)) for x in (own_sum, own_square)]
    sums[me] = jnp.concatenate(own_sums, 1)
    sum_copies = send_all(3, sums)
    for p in range(4):
        for copy in part_copies(p):
            copy.wait_send()
    for core in beside:
        gate_copy(core).wait_send()
    for copies in (att_copies, mix_copies, f_copies):
        for copy in copies:
            copy.wait_send()
    for chip, core in near_peers:
        wait_from(3, sums, chip, core)
    all_sums = functools.reduce(lambda a, b: a + b, [sums[p] for p in range(group)])
    mean = all_sums[:, :128] / width
    var = all_sums[:, 128:] / width - mean * mean
    scale = lax.rsqrt(var + 1e-05)
    mean, scale = [jnp.concatenate([x] * (cols // 128), 1) for x in (mean, scale)]
    out_v[...] = ((summed - mean) * scale * gout[:, own_lanes]).astype(BF16)

    for copy in sum_copies:
        copy.wait_send()


def store_kernel(out_v, nst_v, out_h, nst_h, sem):
    copies = [
        pltpu.make_async_copy(nst_v, nst_h, sem.at[0]),
        pltpu.make_async_copy(out_v, out_h, sem.at[1]),
    ]
    for copy in copies:
        copy.start()
    for copy in copies:
        copy.wait()


def fused_step(
    tokens,
    positions,
    state,
    w_query,
    w_key,
    w_value,
    w_gate,
    w_out,
    gain_mix,
    w_ffn_gate,
    w_ffn_up,
    w_ffn_down,
    gain_out,
):
    kv_count = lax.axis_size("kv")
    tp_count = lax.axis_size("tp")
    group = kv_count * tp_count
    rows = tokens.shape[0]
    _, heads, width_head, _ = state.shape
    width = w_ffn_gate.shape[0]
    cols = w_out.shape[1]
    half = width_head // 2
    inverse = 10000.0 ** (-np.arange(half, dtype=np.float32) / half)
    inverse = np.tile(inverse.astype(np.float32), 2)[None, :]
    arrays = (
        tokens,
        positions[None, :],
        state[0],
        w_query,
        w_key,
        w_value,
        w_gate,
        w_out,
        gain_mix[None, :],
        w_ffn_gate.T,
        w_ffn_up.T,
        w_ffn_down,
        gain_out[None, :],
        jnp.asarray(inverse),
    )
    held = [pltpu.VMEM(a.shape, a.dtype) for a in arrays]
    held[9:11] = [pltpu.VMEM((2, w_ffn_gate.shape[1], width), BF16)]
    vmem_spec = pl.BlockSpec(memory_space=pltpu.VMEM)
    any_spec = pl.BlockSpec(memory_space=pl.ANY)
    out, new_state = pl.pallas_call(
        functools.partial(step_kernel, kv_count, tp_count),
        out_shape=(
            pltpu.VMEM((rows, cols), BF16),
            pltpu.VMEM(state.shape[1:], F32),
        ),
        in_specs=[any_spec] * len(arrays),
        out_specs=(vmem_spec, vmem_spec),
        scratch_shapes=held
        + [
            pltpu.VMEM((kv_count, 3, heads, width_head), F32),
            pltpu.VMEM((kv_count, 3, heads, width_head), F32),
            pltpu.VMEM((rows, heads * width_head), F32),
            pltpu.VMEM((rows, cols), F32),
            pltpu.VMEM((kv_count, rows, heads * width_head), F32),
            pltpu.VMEM((tp_count, rows, heads * width_head), F32),
            pltpu.VMEM((group, heads, width_head), F32),
            pltpu.VMEM((group, rows, cols), BF16),
            pltpu.VMEM((8, width), F32),
            pltpu.VMEM((8, w_ffn_gate.shape[1]), F32),
            pltpu.VMEM((8, w_ffn_gate.shape[1]), F32),
            pltpu.VMEM((2 * (kv_count - 1), tp_count * cols, w_ffn_gate.shape[1]), BF16),
            pltpu.VMEM((256, 256), BF16),
            pltpu.VMEM((rows, w_ffn_gate.shape[1]), BF16),
            pltpu.VMEM((group, rows, cols), BF16),
            pltpu.VMEM((group, rows, cols), BF16),
            pltpu.VMEM((group, rows, 256), F32),
        ],
        compiler_params=pltpu.CompilerParams(
            collective_id=0, has_side_effects=True, vmem_limit_bytes=63 * 2**20
        ),
    )(*arrays)
    out, new_state = pl.pallas_call(
        store_kernel,
        out_shape=(
            jax.ShapeDtypeStruct(out.shape, out.dtype),
            jax.ShapeDtypeStruct(new_state.shape, new_state.dtype),
        ),
        in_specs=[vmem_spec, vmem_spec],
        out_specs=(any_spec, any_spec),
        scratch_shapes=[pltpu.SemaphoreType.DMA((2,))],
        compiler_params=pltpu.CompilerParams(vmem_limit_bytes=2**20),
    )(out, new_state)
    return out, new_state[None]


def fits_kernel(tokens, state, w_out, kv_count, tp_count):
    seqs, _, width_head, _ = state.shape
    return (
        seqs == 1
        and width_head == 128
        and w_out.shape[1] % 256 == 0
        and tokens.shape[0] == kv_count
        and 3 <= kv_count <= 6
        and tp_count >= 2
        and kv_count * tp_count <= 16
    )


def rotate(vectors, positions):
    half = vectors.shape[-1] // 2
    inverse = 10000.0 ** (-jnp.arange(half, dtype=jnp.float32) / half)
    angle = positions.astype(jnp.float32)[:, None, None] * inverse[None, None, :]
    cosine = jnp.cos(angle)
    sine = jnp.sin(angle)
    first = vectors[..., :half]
    second = vectors[..., half:]
    return jnp.concatenate([first * cosine - second * sine, first * sine + second * cosine], -1)


def finish_norm(values, sums, squares, count, gain):
    mean = sums / count
    var = squares / count - mean * mean
    return (values - mean[:, None]) * lax.rsqrt(var + 1e-05)[:, None] * gain[None, :]


def on_device(
    tokens,
    positions,
    state,
    w_query,
    w_key,
    w_value,
    w_gate,
    w_out,
    gain_mix,
    w_ffn_gate,
    w_ffn_up,
    w_ffn_down,
    gain_out,
):
    if fits_kernel(tokens, state, w_out, lax.axis_size("kv"), lax.axis_size("tp")):
        return fused_step(
            tokens,
            positions,
            state,
            w_query,
            w_key,
            w_value,
            w_gate,
            w_out,
            gain_mix,
            w_ffn_gate,
            w_ffn_up,
            w_ffn_down,
            gain_out,
        )
    seqs = state.shape[0]
    heads = state.shape[1]
    width_head = state.shape[2]
    proj_cols = w_query.shape[1]
    width = w_ffn_gate.shape[0]
    cols = w_out.shape[1]
    group_rows = tokens.shape[0]
    kv_count = lax.axis_size("kv")
    tp_count = lax.axis_size("tp")
    tp_index = lax.axis_index("tp")
    col_start = (lax.axis_index("kv") * tp_count + tp_index) * cols
    projected = lax.psum_scatter(
        jnp.concatenate(
            [
                jnp.dot(tokens, w_query, preferred_element_type=jnp.float32),
                jnp.dot(tokens, w_key, preferred_element_type=jnp.float32),
                jnp.dot(tokens, w_value, preferred_element_type=jnp.float32),
                jnp.dot(tokens, w_gate, preferred_element_type=jnp.float32),
            ],
            axis=1,
        ),
        "kv",
        scatter_dimension=0,
        tiled=True,
    )
    query = projected[:, :proj_cols].reshape(seqs, heads, width_head)
    key = projected[:, proj_cols : 2 * proj_cols].reshape(seqs, heads, width_head)
    value = projected[:, 2 * proj_cols : 3 * proj_cols].reshape(seqs, heads, width_head)
    gate_pre = projected[:, 3 * proj_cols :]
    query = rotate(query, positions)
    key = rotate(key, positions) * width_head ** (-0.5)
    total_heads = heads * tp_count
    head_ids = (tp_index * heads + jnp.arange(heads, dtype=jnp.int32)).astype(jnp.float32)
    decay = 1.0 - 2.0 ** (-5.0 - 6.0 * head_ids / (total_heads - 1))
    new_state = decay[None, :, None, None] * state + key[:, :, :, None] * value[:, :, None, :]
    retained = jnp.einsum("bhd,bhdv->bhv", query, new_state, precision=lax.Precision.HIGHEST)
    mean = jnp.mean(retained, -1, keepdims=True)
    var = jnp.mean(jnp.square(retained - mean), -1, keepdims=True)
    normed = (retained - mean) * lax.rsqrt(var + 1e-05)
    attended = (normed.reshape(seqs, proj_cols) * jax.nn.silu(gate_pre)).astype(jnp.bfloat16)
    gathered = lax.all_gather(attended[None], ("kv", "tp"), axis=0, tiled=True)
    gathered = gathered.reshape(kv_count, tp_count, seqs, proj_cols)
    out_blocks = w_out.reshape(tp_count, proj_cols, cols)
    mixed = jnp.einsum(
        "itsc,tcd->isd", gathered, out_blocks, preferred_element_type=jnp.float32
    ).reshape(group_rows, cols)
    tokens_own = lax.dynamic_slice_in_dim(tokens, tp_index * cols, cols, 1)
    mixed_pre = (tokens_own.astype(jnp.float32) + mixed).astype(jnp.bfloat16)
    gain_out_own = lax.dynamic_slice_in_dim(gain_out, col_start, cols, 0)
    whole_rows = lax.all_gather(mixed_pre, ("kv", "tp"), axis=1, tiled=True).astype(jnp.float32)
    hidden = finish_norm(
        whole_rows, jnp.sum(whole_rows, 1), jnp.sum(whole_rows * whole_rows, 1), width, gain_mix
    ).astype(jnp.bfloat16)
    hidden_own = lax.dynamic_slice_in_dim(hidden, col_start, cols, 1)
    gate = jnp.dot(hidden, w_ffn_gate, preferred_element_type=jnp.float32)
    upward = jnp.dot(hidden, w_ffn_up, preferred_element_type=jnp.float32)
    inner = (jax.nn.silu(gate) * upward).astype(jnp.bfloat16)
    ffn_cols = lax.psum_scatter(
        lax.dot_general(
            w_ffn_down, inner, (((0,), (1,)), ((), ())), preferred_element_type=jnp.float32
        ),
        ("kv", "tp"),
        scatter_dimension=0,
        tiled=True,
    )
    summed = hidden_own.astype(jnp.float32) + ffn_cols.T
    out_sums, out_squares = lax.psum(
        (jnp.sum(summed, 1), jnp.sum(summed * summed, 1)), ("kv", "tp")
    )
    layer_out = finish_norm(summed, out_sums, out_squares, width, gain_out_own).astype(jnp.bfloat16)
    return (layer_out, new_state)


def solution(mesh):
    return jax.shard_map(
        on_device,
        mesh=mesh,
        in_specs=(
            P("dp", "kv"),
            P(("dp", "kv")),
            P(("dp", "kv"), "tp", None, None),
            P("kv", "tp"),
            P("kv", "tp"),
            P("kv", "tp"),
            P("kv", "tp"),
            P(None, ("kv", "tp")),
            P(),
            P(None, ("kv", "tp")),
            P(None, ("kv", "tp")),
            P(("kv", "tp"), None),
            P(),
        ),
        out_specs=(P("dp", ("kv", "tp")), P(("dp", "kv"), "tp", None, None)),
        check_vma=False,
    )
```

```python
import functools

import jax
import jax.numpy as jnp
import numpy as np
from jax import lax
from jax.experimental import pallas as pl
from jax.experimental.pallas import tpu as pltpu
from jax.sharding import PartitionSpec as P

MESH = pl.DeviceIdType.MESH
F32 = jnp.float32
BF16 = jnp.bfloat16


def dot_rows(values, weight):
    return lax.dot_general(values, weight, (((1,), (1,)), ((), ())), preferred_element_type=F32)


def nearest(kv, count, k):
    low = jnp.minimum(kv, count - 1 - kv)
    step = jnp.where(2 * kv < count, 1, -1)
    side = 1 - 2 * (k % 2)
    return kv + jnp.where(k <= 2 * low, (k + 1) // 2 * side, (k - low) * step)


def step_kernel(kv_count, tp_count, *refs):
    def body(*sems):
        step_body(kv_count, tp_count, *refs, *sems)

    group = kv_count * tp_count
    pl.run_scoped(
        body,
        pltpu.SemaphoreType.DMA((13,)),
        pltpu.SemaphoreType.DMA((kv_count, 2)),
        pltpu.SemaphoreType.DMA((4, kv_count)),
        pltpu.SemaphoreType.DMA((4, kv_count)),
        pltpu.SemaphoreType.DMA((2, tp_count)),
        pltpu.SemaphoreType.DMA((4, group)),
        pltpu.SemaphoreType.DMA((4, group)),
    )


def step_body(
    kv_count,
    tp_count,
    tok_h,
    pos,
    state_h,
    wq_h,
    wk_h,
    wv_h,
    wg_h,
    wout_h,
    gmix_h,
    wfg_h,
    wfu_h,
    wfd_h,
    gout_h,
    inv_h,
    out_v,
    nst,
    tok,
    state,
    wq,
    wk,
    wv,
    wg,
    wout,
    gmix,
    w_up,
    wfd,
    gout,
    inv,
    qsend,
    qrecv,
    half_part,
    mixed_part,
    gate_recv,
    gates,
    att,
    mix,
    gain_rows,
    acc_gate,
    acc_up,
    turned,
    eye,
    inner,
    fsend,
    frecv,
    sums,
    local_sem,
    up_sem,
    q_send_sem,
    q_recv_sem,
    gate_sem,
    send_sem,
    recv_sem,
):
    group = kv_count * tp_count
    dp = lax.axis_index("dp")
    kv = lax.axis_index("kv")
    tp = lax.axis_index("tp")
    me = kv * tp_count + tp
    rows = tok.shape[0]
    heads = state.shape[0]
    width_head = state.shape[1]
    width = w_up.shape[2]
    cols = mix.shape[2]
    ff = w_up.shape[1]

    near = [nearest(kv, kv_count, k) for k in range(1, kv_count)]
    beside = [lax.rem(tp + e, tp_count) for e in range(1, tp_count)]
    far_peers = [(chip, core) for chip in reversed(near) for core in range(tp_count)]
    near_peers = [(kv, core) for core in beside]
    near_peers += [(chip, core) for chip in near for core in range(tp_count)]

    loads = []

    def load(src, dst):
        copy = pltpu.make_async_copy(src, dst, local_sem.at[len(loads)])
        copy.start()
        loads.append(copy)
        return copy

    tok_load = load(tok_h, tok)
    deep = wg.shape[0] // 2
    halves = [pl.ds(0, deep), pl.ds(deep, deep)]
    proj_loads = [[load(src, dst)] for src, dst in ((wq_h, wq), (wk_h, wk), (wv_h, wv))]
    proj_loads.append([load(wg_h.at[half], wg.at[half]) for half in halves])
    inv_load = load(inv_h, inv)
    state_load = load(state_h, state)
    gmix_load = load(gmix_h, gmix)
    gout_load = load(gout_h, gout)

    barrier = pltpu.get_barrier_semaphore()
    for chip, core in far_peers + [(kv, core) for core in beside]:
        pl.semaphore_signal(barrier, inc=1, device_id=(dp, chip, core), device_id_type=MESH)

    eye[...] = jnp.where(
        lax.broadcasted_iota(jnp.int32, eye.shape, 0)
        == lax.broadcasted_iota(jnp.int32, eye.shape, 1),
        1.0,
        0.0,
    ).astype(BF16)
    tok_load.wait()
    later = []

    def part_copies(p):
        return [
            pltpu.make_async_remote_copy(
                src_ref=qsend.at[chip, p] if p < 3 else half_part,
                dst_ref=qrecv.at[kv, p] if p < 3 else gate_recv.at[kv],
                send_sem=q_send_sem.at[p, d],
                recv_sem=q_recv_sem.at[p, kv],
                device_id=(dp, chip, tp),
                device_id_type=MESH,
            )
            for d, chip in reversed(list(enumerate(near)))
        ]

    span = tp_count * cols

    def chip_lanes(chip):
        return pl.ds(pl.multiple_of(chip * span, span), span)

    def up_copy(rank, m):
        chip = nearest(kv, kv_count, kv_count - 1 - rank)
        at = chip_lanes(chip)
        source = (wfg_h, wfu_h)[m] if isinstance(m, int) else wfg_h
        return pltpu.make_async_copy(source.at[:, at], w_up.at[m, :, at], up_sem.at[rank, m])

    stage = jnp.minimum(kv_count - 1 - kv, 3)
    for p, weight in enumerate((wq, wk, wv, wg)):
        proj_loads[p][0].wait()
        if p == 0:
            later.append(load(wout_h, wout))
        ranks = [p] if p < 3 else list(range(3, kv_count))
        for rank in ranks:
            for m in range(2):
                up_copy(rank, m).start()
        if p < 3:
            part = jnp.dot(tok[...], weight[...], preferred_element_type=F32)
        else:
            later.append(load(wfd_h, wfd))
            half_part[...] = jnp.dot(
                tok[:, :deep], weight[:deep], preferred_element_type=F32
            )
            proj_loads[p][1].wait()
            half_part[...] += jnp.dot(
                tok[:, deep:], weight[deep:], preferred_element_type=F32
            )
        for i in range(kv_count if p < 3 else 0):
            for h in range(heads):
                qsend[i, p, h : h + 1, :] = part[
                    i : i + 1, h * width_head : (h + 1) * width_head
                ]

        @pl.when(stage == p)
        def first_sends():
            pl.semaphore_wait(barrier, group - 1)
            for done in range(min(p, 2) + 1):
                for copy in part_copies(done):
                    copy.start()

        if 0 < p < 3:

            @pl.when(stage < p)
            def next_send():
                for copy in part_copies(p):
                    copy.start()

    wout_load, wfd_load = later

    head_id = (tp * heads + lax.broadcasted_iota(jnp.int32, (heads, width_head), 0)).astype(F32)
    total_heads = heads * tp_count
    decay = 1.0 - jnp.exp2(-5.0 - 6.0 * head_id / (total_heads - 1))

    gmix_load.wait()
    gain = gmix[...]
    gain_high = gain.astype(BF16).astype(F32)
    row_id = lax.broadcasted_iota(jnp.int32, (8, width), 0)
    gain_rows[...] = jnp.where(
        row_id == rows, gain_high, jnp.where(row_id == rows + 1, gain - gain_high, 0.0)
    )

    def rotate_row(x):
        return x * cosine + pltpu.roll(x, width_head // 2, 1) * sine

    def collect(p):
        total = qsend[kv, p] if p < 3 else half_part[...]
        for chip in near:
            landed = qrecv.at[chip, p] if p < 3 else gate_recv.at[chip]
            pltpu.make_async_remote_copy(
                src_ref=landed,
                dst_ref=landed,
                send_sem=q_send_sem.at[p, 0],
                recv_sem=q_recv_sem.at[p, chip],
                device_id=(dp, chip, tp),
                device_id_type=MESH,
            ).wait_recv()
            total = total + landed[...]
        return total

    pieces = 2 * (kv_count - 1)

    def by_kv(values):
        return functools.reduce(
            lambda a, b: a + b, [jnp.where(kv == c, n, 0) for c, n in enumerate(values)]
        )

    middle = [pieces // 3] * (kv_count - 2)
    turns = [by_kv([2]), by_kv([pieces - 1] + middle + [1])]
    turns.append(by_kv([pieces] + [n + 2 for n in middle] + [3]))

    def turn(piece, carry):
        rank = piece // 2
        m = piece % 2
        up_copy(rank, m).wait()
        start = nearest(kv, kv_count, kv_count - 1 - rank) * span
        for k in range(0, span, 512):
            for f in range(0, ff, 256):
                n = min(256, ff - f)
                at = pl.ds(pl.multiple_of(start + k, 256), 256)
                turned[piece, k : k + 256, f : f + n] = dot_rows(
                    eye[...], w_up[m, f : f + n, at]
                ).astype(BF16)
                if k + 256 < span:
                    at = pl.ds(pl.multiple_of(start + k + 256, 256), 256)
                    turned[piece, k + 256 : k + 512, f : f + n] = w_up[m, f : f + n, at].T
        return carry

    lax.fori_loop(0, turns[0], turn, 0)
    for copy in part_copies(3):
        copy.start()
    inv_load.wait()
    lane = lax.broadcasted_iota(jnp.int32, (1, width_head), 1)
    angle = pos[0].astype(F32) * inv[...]
    cosine = jnp.cos(angle)
    sine = jnp.sin(angle)
    sine = jnp.where(lane < width_head // 2, -sine, sine)

    lax.fori_loop(turns[0], turns[1], turn, 0)

    state_load.wait()
    query = rotate_row(collect(0))
    query_t = jnp.transpose(query)
    held = jnp.concatenate(
        [
            jnp.sum(query_t[:, h : h + 1] * state[h], axis=0, keepdims=True)
            for h in range(heads)
        ],
        axis=0,
    )
    key = rotate_row(collect(1)) * width_head ** (-0.5)
    match = jnp.sum(query * key, axis=1, keepdims=True)
    value = collect(2)
    retained = decay * held + match * value
    mean = jnp.mean(retained, -1, keepdims=True)
    var = jnp.mean(jnp.square(retained - mean), -1, keepdims=True)
    normed = (retained - mean) * lax.rsqrt(var + 1e-05)
    att[me] = normed

    def remote(phase, src, dst, slot, chip, core):
        return pltpu.make_async_remote_copy(
            src_ref=src,
            dst_ref=dst,
            send_sem=send_sem.at[phase, slot],
            recv_sem=recv_sem.at[phase, me],
            device_id=(dp, chip, core),
            device_id_type=MESH,
        )

    def send_all(phase, ref):
        copies = []
        for chip, core in far_peers + [(kv, core) for core in beside]:
            copy = remote(phase, ref.at[me], ref.at[me], len(copies), chip, core)
            copy.start()
            copies.append(copy)
        return copies

    def wait_from(phase, ref, chip, core):
        source = chip * tp_count + core
        pltpu.make_async_remote_copy(
            src_ref=ref.at[me],
            dst_ref=ref.at[source],
            send_sem=send_sem.at[phase, 0],
            recv_sem=recv_sem.at[phase, source],
            device_id=(dp, chip, core),
            device_id_type=MESH,
        ).wait_recv()

    att_copies = send_all(0, att)

    lax.fori_loop(turns[1], turns[2], turn, 0)

    gate_pre = collect(3)
    gates[tp] = gate_pre / (1.0 + jnp.exp(-gate_pre))

    def gate_copy(core):
        return pltpu.make_async_remote_copy(
            src_ref=gates.at[tp],
            dst_ref=gates.at[tp],
            send_sem=gate_sem.at[0, core],
            recv_sem=gate_sem.at[1, tp],
            device_id=(dp, kv, core),
            device_id_type=MESH,
        )

    for core in beside:
        gate_copy(core).start()


    lax.fori_loop(turns[2], pieces, turn, 0)

    wout_load.wait()
    mixed = None
    for t in reversed(range(tp_count)):
        for chip in near:
            wait_from(0, att, chip, t)

        @pl.when(tp != t)
        def wait_beside():
            wait_from(0, att, kv, t)
            pltpu.make_async_remote_copy(
                src_ref=gates.at[t],
                dst_ref=gates.at[t],
                send_sem=gate_sem.at[0, t],
                recv_sem=gate_sem.at[1, t],
                device_id=(dp, kv, t),
                device_id_type=MESH,
            ).wait_recv()

        lhs = jnp.concatenate(
            [att[pl.ds(t, rows, stride=tp_count), h, :] for h in range(heads)], axis=1
        )
        lhs = (lhs * gates[t]).astype(BF16)
        depth = heads * width_head
        part = jnp.dot(lhs, wout[t * depth : (t + 1) * depth], preferred_element_type=F32)
        if t > 0:
            if t < tp_count - 1:
                part = part + mixed_part[...]
            mixed_part[...] = part
        else:
            mixed = part + mixed_part[...]
    tok_own = tok[:, pl.ds(pl.multiple_of(tp * cols, cols), cols)]
    own = (tok_own.astype(F32) + mixed).astype(BF16)
    mix[me] = own
    mix_copies = send_all(1, mix)

    own = own.astype(F32)
    shift = jnp.mean(own, 1, keepdims=True)
    gout_load.wait()
    for m in range(2):
        up_copy(kv_count - 1, m).wait()
    tile = 256
    starts = list(range(0, ff, tile))
    own_lanes = pl.ds(pl.multiple_of(me * cols, cols), cols)

    def centred(x, lanes):
        z = jnp.concatenate([x * gmix[:, lanes], jnp.zeros((8 - rows, x.shape[1]), F32)], 0)
        return (z + gain_rows[:, lanes]).astype(BF16)

    def up_turned(lhs, rank, depth):
        for start in starts:
            at = pl.ds(start, min(tile, ff - start))
            for m, acc in enumerate((acc_gate, acc_up)):
                acc[:, at] += jnp.dot(
                    lhs, turned[2 * rank + m, depth, at], preferred_element_type=F32
                )

    def up_part(lhs, lanes, first):
        for start in starts:
            at = pl.ds(start, min(tile, ff - start))
            for m, acc in enumerate((acc_gate, acc_up)):
                part = dot_rows(lhs, w_up[m, at, lanes])
                acc[:, at] = part if first else acc[:, at] + part

    own = own - shift
    key_t = jnp.transpose(key)
    for h in range(heads):
        nst[h] = decay[h : h + 1, :] * state[h] + key_t[:, h : h + 1] * value[h : h + 1, :]
    up_part(centred(own, own_lanes), own_lanes, True)
    total = own
    squares = own * own
    for core in beside:
        wait_from(1, mix, kv, core)
        lanes = pl.ds(pl.multiple_of((kv * tp_count + core) * cols, cols), cols)
        x = mix[kv * tp_count + core].astype(F32) - shift
        total = total + x
        squares = squares + x * x
        up_part(centred(x, lanes), lanes, False)
    for k, chip in enumerate(near):
        order = list(reversed(range(tp_count)))
        if k == kv_count - 2:
            wfd_load.wait()
        for part in [[core] for core in order] if k in (0,) else [order]:
            for core in part:
                wait_from(1, mix, chip, core)
            blocks = []
            for core in sorted(part):
                lanes = pl.ds(pl.multiple_of((chip * tp_count + core) * cols, cols), cols)
                x = mix[chip * tp_count + core].astype(F32) - shift
                total = total + x
                squares = squares + x * x
                blocks.append(centred(x, lanes))
            depth = pl.ds(min(part) * cols, len(part) * cols)
            up_turned(jnp.concatenate(blocks, 1), kv_count - 2 - k, depth)

    mean = jnp.sum(total, 1, keepdims=True) / width
    var = jnp.sum(squares, 1, keepdims=True) / width - mean * mean
    scale = lax.rsqrt(var + 1e-05)
    hid_own = ((own - mean) * scale * gmix[:, own_lanes]).astype(BF16).astype(F32)

    def finish(acc, at):
        bias = acc[rows : rows + 1, at] + acc[rows + 1 : rows + 2, at]
        return scale * (acc[:rows, at] - mean * bias)

    for start in starts:
        at = pl.ds(start, min(tile, ff - start))
        gate = finish(acc_gate, at)
        inner[:, at] = (gate / (1.0 + jnp.exp(-gate)) * finish(acc_up, at)).astype(BF16)

    main = ff // 128 * 128

    def down_part(at):
        result = jnp.dot(inner[:, :main], wfd[:main, at], preferred_element_type=F32)
        if main < ff:
            result += jnp.dot(inner[:, main:], wfd[main:, at], preferred_element_type=F32)
        return result

    f_copies = []

    def send_down(chip, core, result):
        owner = chip * tp_count + core
        fsend[owner] = result.astype(BF16)
        copy = remote(2, fsend.at[owner], frecv.at[me], len(f_copies), chip, core)
        copy.start()
        f_copies.append(copy)

    for chip in reversed(near):
        both = down_part(chip_lanes(chip))
        for core in range(tp_count):
            send_down(chip, core, both[:, core * cols : (core + 1) * cols])
    for core in beside:
        lanes = pl.ds(pl.multiple_of((kv * tp_count + core) * cols, cols), cols)
        send_down(kv, core, down_part(lanes))
    summed = hid_own + down_part(own_lanes)
    for chip, core in near_peers:
        wait_from(2, frecv, chip, core)
        summed = summed + frecv[chip * tp_count + core].astype(F32)
    own_sum = jnp.sum(summed, 1, keepdims=True)
    own_square = jnp.sum(summed * summed, 1, keepdims=True)
    own_sums = [jnp.broadcast_to(x, (rows, 128)) for x in (own_sum, own_square)]
    sums[me] = jnp.concatenate(own_sums, 1)
    sum_copies = send_all(3, sums)
    for p in range(4):
        for copy in part_copies(p):
            copy.wait_send()
    for core in beside:
        gate_copy(core).wait_send()
    for copies in (att_copies, mix_copies, f_copies):
        for copy in copies:
            copy.wait_send()
    for chip, core in near_peers:
        wait_from(3, sums, chip, core)
    all_sums = functools.reduce(lambda a, b: a + b, [sums[p] for p in range(group)])
    mean = all_sums[:, :128] / width
    var = all_sums[:, 128:] / width - mean * mean
    scale = lax.rsqrt(var + 1e-05)
    mean, scale = [jnp.concatenate([x] * (cols // 128), 1) for x in (mean, scale)]
    out_v[...] = ((summed - mean) * scale * gout[:, own_lanes]).astype(BF16)

    for copy in sum_copies:
        copy.wait_send()


def store_kernel(out_v, nst_v, out_h, nst_h, sem):
    copies = [
        pltpu.make_async_copy(nst_v, nst_h, sem.at[0]),
        pltpu.make_async_copy(out_v, out_h, sem.at[1]),
    ]
    for copy in copies:
        copy.start()
    for copy in copies:
        copy.wait()


def fused_step(
    tokens,
    positions,
    state,
    w_query,
    w_key,
    w_value,
    w_gate,
    w_out,
    gain_mix,
    w_ffn_gate,
    w_ffn_up,
    w_ffn_down,
    gain_out,
):
    kv_count = lax.axis_size("kv")
    tp_count = lax.axis_size("tp")
    group = kv_count * tp_count
    rows = tokens.shape[0]
    _, heads, width_head, _ = state.shape
    width = w_ffn_gate.shape[0]
    cols = w_out.shape[1]
    half = width_head // 2
    inverse = 10000.0 ** (-np.arange(half, dtype=np.float32) / half)
    inverse = np.tile(inverse.astype(np.float32), 2)[None, :]
    arrays = (
        tokens,
        positions,
        state[0],
        w_query,
        w_key,
        w_value,
        w_gate,
        w_out,
        gain_mix[None, :],
        w_ffn_gate.T,
        w_ffn_up.T,
        w_ffn_down,
        gain_out[None, :],
        jnp.asarray(inverse),
    )
    held = [pltpu.VMEM(a.shape, a.dtype) for a in arrays]
    del held[1]
    held[8:10] = [pltpu.VMEM((2, w_ffn_gate.shape[1], width), BF16)]
    vmem_spec = pl.BlockSpec(memory_space=pltpu.VMEM)
    any_spec = pl.BlockSpec(memory_space=pl.ANY)
    out, new_state = pl.pallas_call(
        functools.partial(step_kernel, kv_count, tp_count),
        out_shape=(
            pltpu.VMEM((rows, cols), BF16),
            pltpu.VMEM(state.shape[1:], F32),
        ),
        in_specs=[any_spec, pl.BlockSpec(memory_space=pltpu.SMEM)]
        + [any_spec] * (len(arrays) - 2),
        out_specs=(vmem_spec, vmem_spec),
        scratch_shapes=held
        + [
            pltpu.VMEM((kv_count, 3, heads, width_head), F32),
            pltpu.VMEM((kv_count, 3, heads, width_head), F32),
            pltpu.VMEM((rows, heads * width_head), F32),
            pltpu.VMEM((rows, cols), F32),
            pltpu.VMEM((kv_count, rows, heads * width_head), F32),
            pltpu.VMEM((tp_count, rows, heads * width_head), F32),
            pltpu.VMEM((group, heads, width_head), F32),
            pltpu.VMEM((group, rows, cols), BF16),
            pltpu.VMEM((8, width), F32),
            pltpu.VMEM((8, w_ffn_gate.shape[1]), F32),
            pltpu.VMEM((8, w_ffn_gate.shape[1]), F32),
            pltpu.VMEM((2 * (kv_count - 1), tp_count * cols, w_ffn_gate.shape[1]), BF16),
            pltpu.VMEM((256, 256), BF16),
            pltpu.VMEM((rows, w_ffn_gate.shape[1]), BF16),
            pltpu.VMEM((group, rows, cols), BF16),
            pltpu.VMEM((group, rows, cols), BF16),
            pltpu.VMEM((group, rows, 256), F32),
        ],
        compiler_params=pltpu.CompilerParams(
            collective_id=0, has_side_effects=True, vmem_limit_bytes=63 * 2**20
        ),
    )(*arrays)
    out, new_state = pl.pallas_call(
        store_kernel,
        out_shape=(
            jax.ShapeDtypeStruct(out.shape, out.dtype),
            jax.ShapeDtypeStruct(new_state.shape, new_state.dtype),
        ),
        in_specs=[vmem_spec, vmem_spec],
        out_specs=(any_spec, any_spec),
        scratch_shapes=[pltpu.SemaphoreType.DMA((2,))],
        compiler_params=pltpu.CompilerParams(vmem_limit_bytes=2**20),
    )(out, new_state)
    return out, new_state[None]


def fits_kernel(tokens, state, w_out, kv_count, tp_count):
    seqs, _, width_head, _ = state.shape
    return (
        seqs == 1
        and width_head == 128
        and w_out.shape[1] % 256 == 0
        and tokens.shape[0] == kv_count
        and 3 <= kv_count <= 6
        and tp_count >= 2
        and kv_count * tp_count <= 16
    )


def rotate(vectors, positions):
    half = vectors.shape[-1] // 2
    inverse = 10000.0 ** (-jnp.arange(half, dtype=jnp.float32) / half)
    angle = positions.astype(jnp.float32)[:, None, None] * inverse[None, None, :]
    cosine = jnp.cos(angle)
    sine = jnp.sin(angle)
    first = vectors[..., :half]
    second = vectors[..., half:]
    return jnp.concatenate([first * cosine - second * sine, first * sine + second * cosine], -1)


def finish_norm(values, sums, squares, count, gain):
    mean = sums / count
    var = squares / count - mean * mean
    return (values - mean[:, None]) * lax.rsqrt(var + 1e-05)[:, None] * gain[None, :]


def on_device(
    tokens,
    positions,
    state,
    w_query,
    w_key,
    w_value,
    w_gate,
    w_out,
    gain_mix,
    w_ffn_gate,
    w_ffn_up,
    w_ffn_down,
    gain_out,
):
    if fits_kernel(tokens, state, w_out, lax.axis_size("kv"), lax.axis_size("tp")):
        return fused_step(
            tokens,
            positions,
            state,
            w_query,
            w_key,
            w_value,
            w_gate,
            w_out,
            gain_mix,
            w_ffn_gate,
            w_ffn_up,
            w_ffn_down,
            gain_out,
        )
    seqs = state.shape[0]
    heads = state.shape[1]
    width_head = state.shape[2]
    proj_cols = w_query.shape[1]
    width = w_ffn_gate.shape[0]
    cols = w_out.shape[1]
    group_rows = tokens.shape[0]
    kv_count = lax.axis_size("kv")
    tp_count = lax.axis_size("tp")
    tp_index = lax.axis_index("tp")
    col_start = (lax.axis_index("kv") * tp_count + tp_index) * cols
    projected = lax.psum_scatter(
        jnp.concatenate(
            [
                jnp.dot(tokens, w_query, preferred_element_type=jnp.float32),
                jnp.dot(tokens, w_key, preferred_element_type=jnp.float32),
                jnp.dot(tokens, w_value, preferred_element_type=jnp.float32),
                jnp.dot(tokens, w_gate, preferred_element_type=jnp.float32),
            ],
            axis=1,
        ),
        "kv",
        scatter_dimension=0,
        tiled=True,
    )
    query = projected[:, :proj_cols].reshape(seqs, heads, width_head)
    key = projected[:, proj_cols : 2 * proj_cols].reshape(seqs, heads, width_head)
    value = projected[:, 2 * proj_cols : 3 * proj_cols].reshape(seqs, heads, width_head)
    gate_pre = projected[:, 3 * proj_cols :]
    query = rotate(query, positions)
    key = rotate(key, positions) * width_head ** (-0.5)
    total_heads = heads * tp_count
    head_ids = (tp_index * heads + jnp.arange(heads, dtype=jnp.int32)).astype(jnp.float32)
    decay = 1.0 - 2.0 ** (-5.0 - 6.0 * head_ids / (total_heads - 1))
    new_state = decay[None, :, None, None] * state + key[:, :, :, None] * value[:, :, None, :]
    retained = jnp.einsum("bhd,bhdv->bhv", query, new_state, precision=lax.Precision.HIGHEST)
    mean = jnp.mean(retained, -1, keepdims=True)
    var = jnp.mean(jnp.square(retained - mean), -1, keepdims=True)
    normed = (retained - mean) * lax.rsqrt(var + 1e-05)
    attended = (normed.reshape(seqs, proj_cols) * jax.nn.silu(gate_pre)).astype(jnp.bfloat16)
    gathered = lax.all_gather(attended[None], ("kv", "tp"), axis=0, tiled=True)
    gathered = gathered.reshape(kv_count, tp_count, seqs, proj_cols)
    out_blocks = w_out.reshape(tp_count, proj_cols, cols)
    mixed = jnp.einsum(
        "itsc,tcd->isd", gathered, out_blocks, preferred_element_type=jnp.float32
    ).reshape(group_rows, cols)
    tokens_own = lax.dynamic_slice_in_dim(tokens, tp_index * cols, cols, 1)
    mixed_pre = (tokens_own.astype(jnp.float32) + mixed).astype(jnp.bfloat16)
    gain_out_own = lax.dynamic_slice_in_dim(gain_out, col_start, cols, 0)
    whole_rows = lax.all_gather(mixed_pre, ("kv", "tp"), axis=1, tiled=True).astype(jnp.float32)
    hidden = finish_norm(
        whole_rows, jnp.sum(whole_rows, 1), jnp.sum(whole_rows * whole_rows, 1), width, gain_mix
    ).astype(jnp.bfloat16)
    hidden_own = lax.dynamic_slice_in_dim(hidden, col_start, cols, 1)
    gate = jnp.dot(hidden, w_ffn_gate, preferred_element_type=jnp.float32)
    upward = jnp.dot(hidden, w_ffn_up, preferred_element_type=jnp.float32)
    inner = (jax.nn.silu(gate) * upward).astype(jnp.bfloat16)
    ffn_cols = lax.psum_scatter(
        lax.dot_general(
            w_ffn_down, inner, (((0,), (1,)), ((), ())), preferred_element_type=jnp.float32
        ),
        ("kv", "tp"),
        scatter_dimension=0,
        tiled=True,
    )
    summed = hidden_own.astype(jnp.float32) + ffn_cols.T
    out_sums, out_squares = lax.psum(
        (jnp.sum(summed, 1), jnp.sum(summed * summed, 1)), ("kv", "tp")
    )
    layer_out = finish_norm(summed, out_sums, out_squares, width, gain_out_own).astype(jnp.bfloat16)
    return (layer_out, new_state)


def solution(mesh):
    return jax.shard_map(
        on_device,
        mesh=mesh,
        in_specs=(
            P("dp", "kv"),
            P(("dp", "kv")),
            P(("dp", "kv"), "tp", None, None),
            P("kv", "tp"),
            P("kv", "tp"),
            P("kv", "tp"),
            P("kv", "tp"),
            P(None, ("kv", "tp")),
            P(),
            P(None, ("kv", "tp")),
            P(None, ("kv", "tp")),
            P(("kv", "tp"), None),
            P(),
        ),
        out_specs=(P("dp", ("kv", "tp")), P(("dp", "kv"), "tp", None, None)),
        check_vma=False,
    )
```

```python
import functools

import jax
import jax.numpy as jnp
import numpy as np
from jax import lax
from jax.experimental import pallas as pl
from jax.experimental.pallas import tpu as pltpu
from jax.sharding import PartitionSpec as P

MESH = pl.DeviceIdType.MESH
F32 = jnp.float32
BF16 = jnp.bfloat16


def dot_rows(values, weight):
    return lax.dot_general(values, weight, (((1,), (1,)), ((), ())), preferred_element_type=F32)


def nearest(kv, count, k):
    low = jnp.minimum(kv, count - 1 - kv)
    step = jnp.where(2 * kv < count, 1, -1)
    side = 1 - 2 * (k % 2)
    return kv + jnp.where(k <= 2 * low, (k + 1) // 2 * side, (k - low) * step)


def step_kernel(kv_count, tp_count, *refs):
    def body(*sems):
        step_body(kv_count, tp_count, *refs, *sems)

    group = kv_count * tp_count
    pl.run_scoped(
        body,
        pltpu.SemaphoreType.DMA((13,)),
        pltpu.SemaphoreType.DMA((kv_count, 2)),
        pltpu.SemaphoreType.DMA((4, kv_count)),
        pltpu.SemaphoreType.DMA((4, kv_count)),
        pltpu.SemaphoreType.DMA((2, tp_count)),
        pltpu.SemaphoreType.DMA((4, group)),
        pltpu.SemaphoreType.DMA((4, group)),
    )


def step_body(
    kv_count,
    tp_count,
    tok_h,
    pos_h,
    state_h,
    wq_h,
    wk_h,
    wv_h,
    wg_h,
    wout_h,
    gmix_h,
    wfg_h,
    wfu_h,
    wfd_h,
    gout_h,
    inv_h,
    out_v,
    nst,
    tok,
    pos,
    state,
    wq,
    wk,
    wv,
    wg,
    wout,
    gmix,
    w_up,
    wfd,
    gout,
    inv,
    qsend,
    qrecv,
    half_part,
    mixed_part,
    gate_recv,
    gates,
    att,
    mix,
    gain_rows,
    acc_gate,
    acc_up,
    turned,
    eye,
    inner,
    fsend,
    frecv,
    sums,
    local_sem,
    up_sem,
    q_send_sem,
    q_recv_sem,
    gate_sem,
    send_sem,
    recv_sem,
):
    group = kv_count * tp_count
    dp = lax.axis_index("dp")
    kv = lax.axis_index("kv")
    tp = lax.axis_index("tp")
    me = kv * tp_count + tp
    rows = tok.shape[0]
    heads = state.shape[0]
    width_head = state.shape[1]
    width = w_up.shape[2]
    cols = mix.shape[2]
    ff = w_up.shape[1]

    near = [nearest(kv, kv_count, k) for k in range(1, kv_count)]
    beside = [lax.rem(tp + e, tp_count) for e in range(1, tp_count)]
    far_peers = [(chip, core) for chip in reversed(near) for core in range(tp_count)]
    near_peers = [(kv, core) for core in beside]
    near_peers += [(chip, core) for chip in near for core in range(tp_count)]

    loads = []

    def load(src, dst):
        copy = pltpu.make_async_copy(src, dst, local_sem.at[len(loads)])
        copy.start()
        loads.append(copy)
        return copy

    tok_load = load(tok_h, tok)
    pos_load = load(pos_h, pos)
    inv_load = load(inv_h, inv)
    deep = wg.shape[0] // 2
    halves = [pl.ds(0, deep), pl.ds(deep, deep)]
    proj_loads = [[load(src, dst)] for src, dst in ((wq_h, wq), (wk_h, wk), (wv_h, wv))]
    proj_loads.append([load(wg_h.at[half], wg.at[half]) for half in halves])
    state_load = load(state_h, state)
    gmix_load = load(gmix_h, gmix)
    gout_load = load(gout_h, gout)

    barrier = pltpu.get_barrier_semaphore()
    for chip, core in far_peers + [(kv, core) for core in beside]:
        pl.semaphore_signal(barrier, inc=1, device_id=(dp, chip, core), device_id_type=MESH)

    pos_load.wait()
    inv_load.wait()
    lane = lax.broadcasted_iota(jnp.int32, (1, width_head), 1)
    eye[...] = jnp.where(
        lax.broadcasted_iota(jnp.int32, eye.shape, 0)
        == lax.broadcasted_iota(jnp.int32, eye.shape, 1),
        1.0,
        0.0,
    ).astype(BF16)
    angle = pos[...].astype(F32) * inv[...]
    cosine = jnp.cos(angle)
    sine = jnp.sin(angle)
    sine = jnp.where(lane < width_head // 2, -sine, sine)

    tok_load.wait()
    later = []

    def part_copies(p):
        return [
            pltpu.make_async_remote_copy(
                src_ref=qsend.at[chip, p] if p < 3 else half_part,
                dst_ref=qrecv.at[kv, p] if p < 3 else gate_recv.at[kv],
                send_sem=q_send_sem.at[p, d],
                recv_sem=q_recv_sem.at[p, kv],
                device_id=(dp, chip, tp),
                device_id_type=MESH,
            )
            for d, chip in reversed(list(enumerate(near)))
        ]

    span = tp_count * cols

    def chip_lanes(chip):
        return pl.ds(pl.multiple_of(chip * span, span), span)

    def up_copy(rank, m):
        chip = nearest(kv, kv_count, kv_count - 1 - rank)
        at = chip_lanes(chip)
        source = (wfg_h, wfu_h)[m] if isinstance(m, int) else wfg_h
        return pltpu.make_async_copy(source.at[:, at], w_up.at[m, :, at], up_sem.at[rank, m])

    stage = jnp.minimum(kv_count - 1 - kv, 3)
    for p, weight in enumerate((wq, wk, wv, wg)):
        proj_loads[p][0].wait()
        if p == 0:
            later.append(load(wout_h, wout))
        ranks = [p] if p < 3 else list(range(3, kv_count))
        for rank in ranks:
            for m in range(2):
                up_copy(rank, m).start()
        if p < 3:
            part = jnp.dot(tok[...], weight[...], preferred_element_type=F32)
        else:
            later.append(load(wfd_h, wfd))
            half_part[...] = jnp.dot(
                tok[:, :deep], weight[:deep], preferred_element_type=F32
            )
            proj_loads[p][1].wait()
            half_part[...] += jnp.dot(
                tok[:, deep:], weight[deep:], preferred_element_type=F32
            )
        for i in range(kv_count if p < 3 else 0):
            for h in range(heads):
                qsend[i, p, h : h + 1, :] = part[
                    i : i + 1, h * width_head : (h + 1) * width_head
                ]

        @pl.when(stage == p)
        def first_sends():
            pl.semaphore_wait(barrier, group - 1)
            for done in range(min(p, 2) + 1):
                for copy in part_copies(done):
                    copy.start()

        if 0 < p < 3:

            @pl.when(stage < p)
            def next_send():
                for copy in part_copies(p):
                    copy.start()

    wout_load, wfd_load = later

    head_id = (tp * heads + lax.broadcasted_iota(jnp.int32, (heads, width_head), 0)).astype(F32)
    total_heads = heads * tp_count
    decay = 1.0 - jnp.exp2(-5.0 - 6.0 * head_id / (total_heads - 1))

    gmix_load.wait()
    gain = gmix[...]
    gain_high = gain.astype(BF16).astype(F32)
    row_id = lax.broadcasted_iota(jnp.int32, (8, width), 0)
    gain_rows[...] = jnp.where(
        row_id == rows, gain_high, jnp.where(row_id == rows + 1, gain - gain_high, 0.0)
    )

    def rotate_row(x):
        return x * cosine + pltpu.roll(x, width_head // 2, 1) * sine

    def collect(p):
        total = qsend[kv, p] if p < 3 else half_part[...]
        for chip in near:
            landed = qrecv.at[chip, p] if p < 3 else gate_recv.at[chip]
            pltpu.make_async_remote_copy(
                src_ref=landed,
                dst_ref=landed,
                send_sem=q_send_sem.at[p, 0],
                recv_sem=q_recv_sem.at[p, chip],
                device_id=(dp, chip, tp),
                device_id_type=MESH,
            ).wait_recv()
            total = total + landed[...]
        return total

    pieces = 2 * (kv_count - 1)

    def by_kv(values):
        return functools.reduce(
            lambda a, b: a + b, [jnp.where(kv == c, n, 0) for c, n in enumerate(values)]
        )

    middle = [pieces // 3] * (kv_count - 2)
    turns = [by_kv([2]), by_kv([pieces - 1] + middle + [1])]
    turns.append(by_kv([pieces] + [n + 2 for n in middle] + [3]))

    def turn(piece, carry):
        rank = piece // 2
        m = piece % 2
        up_copy(rank, m).wait()
        start = nearest(kv, kv_count, kv_count - 1 - rank) * span
        for k in range(0, span, 512):
            for f in range(0, ff, 256):
                n = min(256, ff - f)
                at = pl.ds(pl.multiple_of(start + k, 256), 256)
                turned[piece, k : k + 256, f : f + n] = dot_rows(
                    eye[...], w_up[m, f : f + n, at]
                ).astype(BF16)
                if k + 256 < span:
                    at = pl.ds(pl.multiple_of(start + k + 256, 256), 256)
                    turned[piece, k + 256 : k + 512, f : f + n] = w_up[m, f : f + n, at].T
        return carry

    lax.fori_loop(0, turns[0], turn, 0)
    for copy in part_copies(3):
        copy.start()
    lax.fori_loop(turns[0], turns[1], turn, 0)

    state_load.wait()
    query = rotate_row(collect(0))
    query_t = jnp.transpose(query)
    held = jnp.concatenate(
        [
            jnp.sum(query_t[:, h : h + 1] * state[h], axis=0, keepdims=True)
            for h in range(heads)
        ],
        axis=0,
    )
    key = rotate_row(collect(1)) * width_head ** (-0.5)
    match = jnp.sum(query * key, axis=1, keepdims=True)
    value = collect(2)
    retained = decay * held + match * value
    mean = jnp.mean(retained, -1, keepdims=True)
    var = jnp.mean(jnp.square(retained - mean), -1, keepdims=True)
    normed = (retained - mean) * lax.rsqrt(var + 1e-05)
    att[me] = normed

    def remote(phase, src, dst, slot, chip, core):
        return pltpu.make_async_remote_copy(
            src_ref=src,
            dst_ref=dst,
            send_sem=send_sem.at[phase, slot],
            recv_sem=recv_sem.at[phase, me],
            device_id=(dp, chip, core),
            device_id_type=MESH,
        )

    def send_all(phase, ref):
        copies = []
        for chip, core in far_peers + [(kv, core) for core in beside]:
            copy = remote(phase, ref.at[me], ref.at[me], len(copies), chip, core)
            copy.start()
            copies.append(copy)
        return copies

    def wait_from(phase, ref, chip, core):
        source = chip * tp_count + core
        pltpu.make_async_remote_copy(
            src_ref=ref.at[me],
            dst_ref=ref.at[source],
            send_sem=send_sem.at[phase, 0],
            recv_sem=recv_sem.at[phase, source],
            device_id=(dp, chip, core),
            device_id_type=MESH,
        ).wait_recv()

    att_copies = send_all(0, att)

    lax.fori_loop(turns[1], turns[2], turn, 0)

    gate_pre = collect(3)
    gates[tp] = gate_pre / (1.0 + jnp.exp(-gate_pre))

    def gate_copy(core):
        return pltpu.make_async_remote_copy(
            src_ref=gates.at[tp],
            dst_ref=gates.at[tp],
            send_sem=gate_sem.at[0, core],
            recv_sem=gate_sem.at[1, tp],
            device_id=(dp, kv, core),
            device_id_type=MESH,
        )

    for core in beside:
        gate_copy(core).start()

    key_t = jnp.transpose(key)
    for h in range(heads):
        nst[h] = decay[h : h + 1, :] * state[h] + key_t[:, h : h + 1] * value[h : h + 1, :]

    lax.fori_loop(turns[2], pieces, turn, 0)

    wout_load.wait()
    mixed = None
    for t in reversed(range(tp_count)):
        for chip in near:
            wait_from(0, att, chip, t)

        @pl.when(tp != t)
        def wait_beside():
            wait_from(0, att, kv, t)
            pltpu.make_async_remote_copy(
                src_ref=gates.at[t],
                dst_ref=gates.at[t],
                send_sem=gate_sem.at[0, t],
                recv_sem=gate_sem.at[1, t],
                device_id=(dp, kv, t),
                device_id_type=MESH,
            ).wait_recv()

        lhs = jnp.concatenate(
            [att[pl.ds(t, rows, stride=tp_count), h, :] for h in range(heads)], axis=1
        )
        lhs = (lhs * gates[t]).astype(BF16)
        depth = heads * width_head
        part = jnp.dot(lhs, wout[t * depth : (t + 1) * depth], preferred_element_type=F32)
        if t > 0:
            if t < tp_count - 1:
                part = part + mixed_part[...]
            mixed_part[...] = part
        else:
            mixed = part + mixed_part[...]
    tok_own = tok[:, pl.ds(pl.multiple_of(tp * cols, cols), cols)]
    own = (tok_own.astype(F32) + mixed).astype(BF16)
    mix[me] = own
    mix_copies = send_all(1, mix)

    own = own.astype(F32)
    shift = jnp.mean(own, 1, keepdims=True)
    gout_load.wait()
    for m in range(2):
        up_copy(kv_count - 1, m).wait()
    tile = 256
    starts = list(range(0, ff, tile))
    own_lanes = pl.ds(pl.multiple_of(me * cols, cols), cols)

    def centred(x, lanes):
        z = jnp.concatenate([x * gmix[:, lanes], jnp.zeros((8 - rows, x.shape[1]), F32)], 0)
        return (z + gain_rows[:, lanes]).astype(BF16)

    def up_turned(lhs, rank, depth):
        for start in starts:
            at = pl.ds(start, min(tile, ff - start))
            for m, acc in enumerate((acc_gate, acc_up)):
                acc[:, at] += jnp.dot(
                    lhs, turned[2 * rank + m, depth, at], preferred_element_type=F32
                )

    def up_part(lhs, lanes, first):
        for start in starts:
            at = pl.ds(start, min(tile, ff - start))
            for m, acc in enumerate((acc_gate, acc_up)):
                part = dot_rows(lhs, w_up[m, at, lanes])
                acc[:, at] = part if first else acc[:, at] + part

    own = own - shift
    up_part(centred(own, own_lanes), own_lanes, True)
    total = own
    squares = own * own
    for core in beside:
        wait_from(1, mix, kv, core)
        lanes = pl.ds(pl.multiple_of((kv * tp_count + core) * cols, cols), cols)
        x = mix[kv * tp_count + core].astype(F32) - shift
        total = total + x
        squares = squares + x * x
        up_part(centred(x, lanes), lanes, False)
    for k, chip in enumerate(near):
        order = list(reversed(range(tp_count)))
        if k == kv_count - 2:
            wfd_load.wait()
        for part in [[core] for core in order] if k in (0, 1) else [order]:
            for core in part:
                wait_from(1, mix, chip, core)
            blocks = []
            for core in sorted(part):
                lanes = pl.ds(pl.multiple_of((chip * tp_count + core) * cols, cols), cols)
                x = mix[chip * tp_count + core].astype(F32) - shift
                total = total + x
                squares = squares + x * x
                blocks.append(centred(x, lanes))
            depth = pl.ds(min(part) * cols, len(part) * cols)
            up_turned(jnp.concatenate(blocks, 1), kv_count - 2 - k, depth)

    mean = jnp.sum(total, 1, keepdims=True) / width
    var = jnp.sum(squares, 1, keepdims=True) / width - mean * mean
    scale = lax.rsqrt(var + 1e-05)
    hid_own = ((own - mean) * scale * gmix[:, own_lanes]).astype(BF16).astype(F32)

    def finish(acc, at):
        bias = acc[rows : rows + 1, at] + acc[rows + 1 : rows + 2, at]
        return scale * (acc[:rows, at] - mean * bias)

    for start in starts:
        at = pl.ds(start, min(tile, ff - start))
        gate = finish(acc_gate, at)
        inner[:, at] = (gate / (1.0 + jnp.exp(-gate)) * finish(acc_up, at)).astype(BF16)

    main = ff // 128 * 128

    def down_part(at):
        result = jnp.dot(inner[:, :main], wfd[:main, at], preferred_element_type=F32)
        if main < ff:
            result += jnp.dot(inner[:, main:], wfd[main:, at], preferred_element_type=F32)
        return result

    f_copies = []

    def send_down(chip, core, result):
        owner = chip * tp_count + core
        fsend[owner] = result.astype(BF16)
        copy = remote(2, fsend.at[owner], frecv.at[me], len(f_copies), chip, core)
        copy.start()
        f_copies.append(copy)

    for chip in reversed(near):
        both = down_part(chip_lanes(chip))
        for core in range(tp_count):
            send_down(chip, core, both[:, core * cols : (core + 1) * cols])
    for core in beside:
        lanes = pl.ds(pl.multiple_of((kv * tp_count + core) * cols, cols), cols)
        send_down(kv, core, down_part(lanes))
    summed = hid_own + down_part(own_lanes)
    for chip, core in near_peers:
        wait_from(2, frecv, chip, core)
        summed = summed + frecv[chip * tp_count + core].astype(F32)
    own_sum = jnp.sum(summed, 1, keepdims=True)
    own_square = jnp.sum(summed * summed, 1, keepdims=True)
    own_sums = [jnp.broadcast_to(x, (rows, 128)) for x in (own_sum, own_square)]
    sums[me] = jnp.concatenate(own_sums, 1)
    sum_copies = send_all(3, sums)
    for p in range(4):
        for copy in part_copies(p):
            copy.wait_send()
    for core in beside:
        gate_copy(core).wait_send()
    for copies in (att_copies, mix_copies, f_copies):
        for copy in copies:
            copy.wait_send()
    for chip, core in near_peers:
        wait_from(3, sums, chip, core)
    all_sums = functools.reduce(lambda a, b: a + b, [sums[p] for p in range(group)])
    mean = all_sums[:, :128] / width
    var = all_sums[:, 128:] / width - mean * mean
    scale = lax.rsqrt(var + 1e-05)
    mean, scale = [jnp.concatenate([x] * (cols // 128), 1) for x in (mean, scale)]
    out_v[...] = ((summed - mean) * scale * gout[:, own_lanes]).astype(BF16)

    for copy in sum_copies:
        copy.wait_send()


def store_kernel(out_v, nst_v, out_h, nst_h, sem):
    copies = [
        pltpu.make_async_copy(nst_v, nst_h, sem.at[0]),
        pltpu.make_async_copy(out_v, out_h, sem.at[1]),
    ]
    for copy in copies:
        copy.start()
    for copy in copies:
        copy.wait()


def fused_step(
    tokens,
    positions,
    state,
    w_query,
    w_key,
    w_value,
    w_gate,
    w_out,
    gain_mix,
    w_ffn_gate,
    w_ffn_up,
    w_ffn_down,
    gain_out,
):
    kv_count = lax.axis_size("kv")
    tp_count = lax.axis_size("tp")
    group = kv_count * tp_count
    rows = tokens.shape[0]
    _, heads, width_head, _ = state.shape
    width = w_ffn_gate.shape[0]
    cols = w_out.shape[1]
    half = width_head // 2
    inverse = 10000.0 ** (-np.arange(half, dtype=np.float32) / half)
    inverse = np.tile(inverse.astype(np.float32), 2)[None, :]
    arrays = (
        tokens,
        positions[None, :],
        state[0],
        w_query,
        w_key,
        w_value,
        w_gate,
        w_out,
        gain_mix[None, :],
        w_ffn_gate.T,
        w_ffn_up.T,
        w_ffn_down,
        gain_out[None, :],
        jnp.asarray(inverse),
    )
    held = [pltpu.VMEM(a.shape, a.dtype) for a in arrays]
    held[9:11] = [pltpu.VMEM((2, w_ffn_gate.shape[1], width), BF16)]
    vmem_spec = pl.BlockSpec(memory_space=pltpu.VMEM)
    any_spec = pl.BlockSpec(memory_space=pl.ANY)
    out, new_state = pl.pallas_call(
        functools.partial(step_kernel, kv_count, tp_count),
        out_shape=(
            pltpu.VMEM((rows, cols), BF16),
            pltpu.VMEM(state.shape[1:], F32),
        ),
        in_specs=[any_spec] * len(arrays),
        out_specs=(vmem_spec, vmem_spec),
        scratch_shapes=held
        + [
            pltpu.VMEM((kv_count, 3, heads, width_head), F32),
            pltpu.VMEM((kv_count, 3, heads, width_head), F32),
            pltpu.VMEM((rows, heads * width_head), F32),
            pltpu.VMEM((rows, cols), F32),
            pltpu.VMEM((kv_count, rows, heads * width_head), F32),
            pltpu.VMEM((tp_count, rows, heads * width_head), F32),
            pltpu.VMEM((group, heads, width_head), F32),
            pltpu.VMEM((group, rows, cols), BF16),
            pltpu.VMEM((8, width), F32),
            pltpu.VMEM((8, w_ffn_gate.shape[1]), F32),
            pltpu.VMEM((8, w_ffn_gate.shape[1]), F32),
            pltpu.VMEM((2 * (kv_count - 1), tp_count * cols, w_ffn_gate.shape[1]), BF16),
            pltpu.VMEM((256, 256), BF16),
            pltpu.VMEM((rows, w_ffn_gate.shape[1]), BF16),
            pltpu.VMEM((group, rows, cols), BF16),
            pltpu.VMEM((group, rows, cols), BF16),
            pltpu.VMEM((group, rows, 256), F32),
        ],
        compiler_params=pltpu.CompilerParams(
            collective_id=0, has_side_effects=True, vmem_limit_bytes=63 * 2**20
        ),
    )(*arrays)
    out, new_state = pl.pallas_call(
        store_kernel,
        out_shape=(
            jax.ShapeDtypeStruct(out.shape, out.dtype),
            jax.ShapeDtypeStruct(new_state.shape, new_state.dtype),
        ),
        in_specs=[vmem_spec, vmem_spec],
        out_specs=(any_spec, any_spec),
        scratch_shapes=[pltpu.SemaphoreType.DMA((2,))],
        compiler_params=pltpu.CompilerParams(vmem_limit_bytes=2**20),
    )(out, new_state)
    return out, new_state[None]


def fits_kernel(tokens, state, w_out, kv_count, tp_count):
    seqs, _, width_head, _ = state.shape
    return (
        seqs == 1
        and width_head == 128
        and w_out.shape[1] % 256 == 0
        and tokens.shape[0] == kv_count
        and 3 <= kv_count <= 6
        and tp_count >= 2
        and kv_count * tp_count <= 16
    )


def rotate(vectors, positions):
    half = vectors.shape[-1] // 2
    inverse = 10000.0 ** (-jnp.arange(half, dtype=jnp.float32) / half)
    angle = positions.astype(jnp.float32)[:, None, None] * inverse[None, None, :]
    cosine = jnp.cos(angle)
    sine = jnp.sin(angle)
    first = vectors[..., :half]
    second = vectors[..., half:]
    return jnp.concatenate([first * cosine - second * sine, first * sine + second * cosine], -1)


def finish_norm(values, sums, squares, count, gain):
    mean = sums / count
    var = squares / count - mean * mean
    return (values - mean[:, None]) * lax.rsqrt(var + 1e-05)[:, None] * gain[None, :]


def on_device(
    tokens,
    positions,
    state,
    w_query,
    w_key,
    w_value,
    w_gate,
    w_out,
    gain_mix,
    w_ffn_gate,
    w_ffn_up,
    w_ffn_down,
    gain_out,
):
    if fits_kernel(tokens, state, w_out, lax.axis_size("kv"), lax.axis_size("tp")):
        return fused_step(
            tokens,
            positions,
            state,
            w_query,
            w_key,
            w_value,
            w_gate,
            w_out,
            gain_mix,
            w_ffn_gate,
            w_ffn_up,
            w_ffn_down,
            gain_out,
        )
    seqs = state.shape[0]
    heads = state.shape[1]
    width_head = state.shape[2]
    proj_cols = w_query.shape[1]
    width = w_ffn_gate.shape[0]
    cols = w_out.shape[1]
    group_rows = tokens.shape[0]
    kv_count = lax.axis_size("kv")
    tp_count = lax.axis_size("tp")
    tp_index = lax.axis_index("tp")
    col_start = (lax.axis_index("kv") * tp_count + tp_index) * cols
    projected = lax.psum_scatter(
        jnp.concatenate(
            [
                jnp.dot(tokens, w_query, preferred_element_type=jnp.float32),
                jnp.dot(tokens, w_key, preferred_element_type=jnp.float32),
                jnp.dot(tokens, w_value, preferred_element_type=jnp.float32),
                jnp.dot(tokens, w_gate, preferred_element_type=jnp.float32),
            ],
            axis=1,
        ),
        "kv",
        scatter_dimension=0,
        tiled=True,
    )
    query = projected[:, :proj_cols].reshape(seqs, heads, width_head)
    key = projected[:, proj_cols : 2 * proj_cols].reshape(seqs, heads, width_head)
    value = projected[:, 2 * proj_cols : 3 * proj_cols].reshape(seqs, heads, width_head)
    gate_pre = projected[:, 3 * proj_cols :]
    query = rotate(query, positions)
    key = rotate(key, positions) * width_head ** (-0.5)
    total_heads = heads * tp_count
    head_ids = (tp_index * heads + jnp.arange(heads, dtype=jnp.int32)).astype(jnp.float32)
    decay = 1.0 - 2.0 ** (-5.0 - 6.0 * head_ids / (total_heads - 1))
    new_state = decay[None, :, None, None] * state + key[:, :, :, None] * value[:, :, None, :]
    retained = jnp.einsum("bhd,bhdv->bhv", query, new_state, precision=lax.Precision.HIGHEST)
    mean = jnp.mean(retained, -1, keepdims=True)
    var = jnp.mean(jnp.square(retained - mean), -1, keepdims=True)
    normed = (retained - mean) * lax.rsqrt(var + 1e-05)
    attended = (normed.reshape(seqs, proj_cols) * jax.nn.silu(gate_pre)).astype(jnp.bfloat16)
    gathered = lax.all_gather(attended[None], ("kv", "tp"), axis=0, tiled=True)
    gathered = gathered.reshape(kv_count, tp_count, seqs, proj_cols)
    out_blocks = w_out.reshape(tp_count, proj_cols, cols)
    mixed = jnp.einsum(
        "itsc,tcd->isd", gathered, out_blocks, preferred_element_type=jnp.float32
    ).reshape(group_rows, cols)
    tokens_own = lax.dynamic_slice_in_dim(tokens, tp_index * cols, cols, 1)
    mixed_pre = (tokens_own.astype(jnp.float32) + mixed).astype(jnp.bfloat16)
    gain_out_own = lax.dynamic_slice_in_dim(gain_out, col_start, cols, 0)
    whole_rows = lax.all_gather(mixed_pre, ("kv", "tp"), axis=1, tiled=True).astype(jnp.float32)
    hidden = finish_norm(
        whole_rows, jnp.sum(whole_rows, 1), jnp.sum(whole_rows * whole_rows, 1), width, gain_mix
    ).astype(jnp.bfloat16)
    hidden_own = lax.dynamic_slice_in_dim(hidden, col_start, cols, 1)
    gate = jnp.dot(hidden, w_ffn_gate, preferred_element_type=jnp.float32)
    upward = jnp.dot(hidden, w_ffn_up, preferred_element_type=jnp.float32)
    inner = (jax.nn.silu(gate) * upward).astype(jnp.bfloat16)
    ffn_cols = lax.psum_scatter(
        lax.dot_general(
            w_ffn_down, inner, (((0,), (1,)), ((), ())), preferred_element_type=jnp.float32
        ),
        ("kv", "tp"),
        scatter_dimension=0,
        tiled=True,
    )
    summed = hidden_own.astype(jnp.float32) + ffn_cols.T
    out_sums, out_squares = lax.psum(
        (jnp.sum(summed, 1), jnp.sum(summed * summed, 1)), ("kv", "tp")
    )
    layer_out = finish_norm(summed, out_sums, out_squares, width, gain_out_own).astype(jnp.bfloat16)
    return (layer_out, new_state)


def solution(mesh):
    return jax.shard_map(
        on_device,
        mesh=mesh,
        in_specs=(
            P("dp", "kv"),
            P(("dp", "kv")),
            P(("dp", "kv"), "tp", None, None),
            P("kv", "tp"),
            P("kv", "tp"),
            P("kv", "tp"),
            P("kv", "tp"),
            P(None, ("kv", "tp")),
            P(),
            P(None, ("kv", "tp")),
            P(None, ("kv", "tp")),
            P(("kv", "tp"), None),
            P(),
        ),
        out_specs=(P("dp", ("kv", "tp")), P(("dp", "kv"), "tp", None, None)),
        check_vma=False,
    )
```
